32 devices in a mesh: grp: 2 (over x), ep: 16 (over z, y, core).
Axes of the slice: x: 2, y: 2, z: 4, core: 2. Of those that a mesh axis runs over, the one named last changes fastest.
Arguments:
- tokens: bfloat16 [384, 2048], P(('grp', 'ep')), parts along dimension 0, may hold values from -6 to 6
- norm_gain: float32 [2048], replicated, may hold values from 0.1 to 1.9
- query_weight: bfloat16 [2048, 512], P('ep'), may hold values from -0.125 to 0.125
- key_weight: bfloat16 [2048, 512], P('ep'), may hold values from -0.125 to 0.125
- value_weight: bfloat16 [2048, 512], P('ep'), may hold values from -0.125 to 0.125
- outgate_weight: bfloat16 [2048, 512], P('ep'), may hold values from -0.125 to 0.125
- ingate_weight: bfloat16 [2048, 4], P('ep'), may hold values from -0.125 to 0.125
- forget_weight: bfloat16 [2048, 4], P('ep'), may hold values from -0.125 to 0.125
- ingate_bias: float32 [4], replicated, may hold values from -1 to 1
- forget_bias: float32 [4], replicated, may hold values from 0.5 to 4
- memory: float32 [384, 4, 128, 128], P(('grp', 'ep')), parts along dimension 0, may hold values from -4 to 4
- normalizer: float32 [384, 4, 128], P(('grp', 'ep')), parts along dimension 0, may hold values from -4 to 4
- stabilizer: float32 [384, 4], P(('grp', 'ep')), parts along dimension 0, may hold values from -1 to 2
- mixer_weight: bfloat16 [512, 2048], P(None, 'ep'), may hold values from -0.25 to 0.25
- moe_gain: float32 [2048], replicated, may hold values from 0.1 to 1.9
- expert_gate: bfloat16 [16, 2048, 512], P('ep'), may hold values from -0.125 to 0.125
- expert_up: bfloat16 [16, 2048, 512], P('ep'), may hold values from -0.125 to 0.125
- expert_down: bfloat16 [16, 512, 2048], P('ep'), may hold values from -0.25 to 0.25
- expert_index: int32 [384, 6], P(('grp', 'ep')), parts along dimension 0, may hold values from 0 to 15, as said below
- route_weights: float32 [384, 6], P(('grp', 'ep')), parts along dimension 0, may hold values from 0.1 to 1
Outputs:
- layer_out: bfloat16 [384, 2048], P(('grp', 'ep')), parts along dimension 0
- new_memory: float32 [384, 4, 128, 128], P(('grp', 'ep')), parts along dimension 0
- new_normalizer: float32 [384, 4, 128], P(('grp', 'ep')), parts along dimension 0
- new_stabilizer: float32 [384, 4], P(('grp', 'ep')), parts along dimension 0
The draws below stay inside these ranges and needn't reach their ends.
There are 2 independent parts, one for each index of `grp`. The reference program is written for one: setup_inputs(seed, part) draws one part's arguments, and reference() takes and returns one part's arrays. A program takes and returns all parts, laid end to end along the dimension named above; an argument that names none is the same for every part. Nothing has to cross between parts.
Inputs may be any that keep to these rules, and one draw needn't show every extreme that they name: `expert_index`: experts 0 to 15 form two groups of 8 consecutive numbers; each row names 6 different experts of one group. Among the 12 rows of one device at most 5 name one expert, and in every device some expert is named by exactly 5 of them.
All inputs are finite; a program needn't handle non-finite values.
Results may differ from the reference program's by a relative error of at most 0.013.
Values may be sent and summed in bfloat16 or wider, within the bound.
No kernel may reach another device: no remote copies, remote signals or barrier semaphores. Data moves between devices by JAX's collectives and lax.ppermute only.
A program may use at most 128 MiB of HBM per device.

```python
import math
import jax
import jax.numpy as jnp
from jax import lax

D = 2048
M_HEADS = 4
M_HEAD_DIM = 128
M_WIDTH = 512
D_EXPERT = 512
TOP_K = 6
EXPERTS = 16
SEQ_DEV = 12
TOKENS = 192
CAP = 5
N_EP = 16


def draw_expert_index(key, part):
    blocks = TOKENS // SEQ_DEV
    group_size = EXPERTS // 2
    offsets = jax.random.randint(jax.random.fold_in(key, 21), (blocks, 2), 0, group_size)
    flips = jax.random.randint(jax.random.fold_in(key, 22), (blocks, 1), 0, 2)
    within = jnp.arange(SEQ_DEV, dtype=jnp.int32)
    parity = within % 2
    groups = (parity[None, :] + flips) % 2
    position = within // 2
    starts = jnp.take_along_axis(offsets, groups, axis=1) + position[None, :] * TOP_K
    steps_k = jnp.arange(TOP_K, dtype=jnp.int32)
    chosen = groups[:, :, None] * group_size + (starts[:, :, None] + steps_k[None, None, :]) % group_size
    block_keys = jax.random.split(jax.random.fold_in(key, 23), blocks)
    orders = jax.vmap(lambda single: jax.random.permutation(single, SEQ_DEV))(block_keys)
    chosen = jnp.take_along_axis(chosen, orders[:, :, None], axis=1)
    return chosen.reshape(TOKENS, TOP_K).astype(jnp.int32)


def block_scale(stream_key, dims, pieces, least, top_value):
    loudness, own = 1.0, jax.random.fold_in(stream_key, 6)
    for dim, shards_of in pieces:
        steps = jnp.exp(jax.random.uniform(jax.random.fold_in(own, dim), (shards_of,), jnp.float32, least / len(pieces), top_value / len(pieces)))
        loudness = loudness * jnp.repeat(steps, dims[dim] // shards_of).reshape([-1 if axis == dim else 1 for axis in range(len(dims))])
    return loudness


def gaussian(rng, dims, spread, most, pieces=(), kind=jnp.bfloat16):
    level = block_scale(rng, dims, pieces, -0.22, 0.18) if pieces else 1.0
    values = jax.random.normal(rng, dims, jnp.float32) * spread * level
    return jnp.minimum(jnp.maximum(values, -most), most).astype(kind)


def setup_inputs(seed: int = 0, part: int = 0) -> dict:
    streams_of = jax.random.split(jax.random.key(seed), 21)
    own_keys = jax.random.split(jax.random.fold_in(streams_of[20], part), 21)
    tokens = gaussian(own_keys[0], (TOKENS, D), 1.0, 6.0, ((0, 16),))
    norm_gain = jnp.clip(1.0 + 0.18 * jax.random.normal(streams_of[1], (D,), jnp.float32), 0.1, 1.9)
    query_weight = gaussian(streams_of[2], (D, M_WIDTH), D ** -0.5, 0.125, ((0, 16),))
    key_weight = gaussian(streams_of[3], (D, M_WIDTH), D ** -0.5, 0.125, ((0, 16),))
    value_weight = gaussian(streams_of[4], (D, M_WIDTH), D ** -0.5, 0.125, ((0, 16),))
    outgate_weight = gaussian(streams_of[5], (D, M_WIDTH), D ** -0.5, 0.125, ((0, 16),))
    ingate_weight = gaussian(streams_of[6], (D, M_HEADS), D ** -0.5, 0.125, ((0, 16),))
    forget_weight = gaussian(streams_of[7], (D, M_HEADS), D ** -0.5, 0.125, ((0, 16),))
    ingate_bias = jnp.clip(jax.random.uniform(streams_of[8], (M_HEADS,), jnp.float32, -1.0, 1.0), -1.0, 1.0)
    forget_bias = jnp.clip(jax.random.uniform(streams_of[9], (M_HEADS,), jnp.float32, 0.5, 4.0), 0.5, 4.0)
    memory = gaussian(own_keys[10], (TOKENS, M_HEADS, M_HEAD_DIM, M_HEAD_DIM), 0.3, 4.0, ((0, 16),), jnp.float32)
    normalizer = gaussian(own_keys[11], (TOKENS, M_HEADS, M_HEAD_DIM), 0.3, 4.0, ((0, 16),), jnp.float32)
    stabilizer = jnp.clip(-1.0 + 3.0 * jax.random.uniform(own_keys[12], (TOKENS, M_HEADS), jnp.float32) ** block_scale(own_keys[12], (TOKENS, M_HEADS), ((0, 16),), -0.2, 0.2), -1.0, 2.0)
    mixer_weight = gaussian(streams_of[13], (M_WIDTH, D), M_WIDTH ** -0.5, 0.25, ((1, 16),))
    moe_gain = jnp.clip(1.0 + 0.18 * jax.random.normal(streams_of[14], (D,), jnp.float32), 0.1, 1.9)
    expert_gate = gaussian(streams_of[15], (EXPERTS, D, D_EXPERT), D ** -0.5, 0.125, ((0, 16),))
    expert_up = gaussian(streams_of[16], (EXPERTS, D, D_EXPERT), D ** -0.5, 0.125, ((0, 16),))
    expert_down = gaussian(streams_of[17], (EXPERTS, D_EXPERT, D), D_EXPERT ** -0.5, 0.25, ((0, 16),))
    expert_index = draw_expert_index(jax.random.fold_in(jax.random.fold_in(streams_of[20], part), 71), part)
    route_weights = jnp.clip(jnp.exp(math.log(1.0) - 2.3025851 * jax.random.uniform(own_keys[19], (TOKENS, TOP_K), jnp.float32) ** block_scale(own_keys[19], (TOKENS, TOP_K), ((0, 16),), -0.2, 0.2)), 0.1, 1.0)
    return {"tokens": tokens, "norm_gain": norm_gain, "query_weight": query_weight, "key_weight": key_weight, "value_weight": value_weight, "outgate_weight": outgate_weight, "ingate_weight": ingate_weight, "forget_weight": forget_weight, "ingate_bias": ingate_bias, "forget_bias": forget_bias, "memory": memory, "normalizer": normalizer, "stabilizer": stabilizer, "mixer_weight": mixer_weight, "moe_gain": moe_gain, "expert_gate": expert_gate, "expert_up": expert_up, "expert_down": expert_down, "expert_index": expert_index, "route_weights": route_weights}


EPS = 1e-06

def rms_normed(values, gain):
    scale = lax.rsqrt(lax.optimization_barrier(jnp.mean(values * values, axis=-1, keepdims=True)) + EPS)
    return values * scale * gain

def reference(tokens, norm_gain, query_weight, key_weight, value_weight, outgate_weight, ingate_weight, forget_weight, ingate_bias, forget_bias, memory, normalizer, stabilizer, mixer_weight, moe_gain, expert_gate, expert_up, expert_down, expert_index, route_weights):
    f32 = jnp.float32
    bf16 = jnp.bfloat16
    stream = tokens.astype(f32)
    normed = rms_normed(stream, norm_gain).astype(bf16)

    def project(weight):
        return jnp.dot(normed, weight, preferred_element_type=f32)
    queries = project(query_weight).astype(bf16)
    key_rows = project(key_weight).astype(bf16)
    value_rows = project(value_weight).astype(bf16)
    outgate = project(outgate_weight).astype(bf16)
    ingate_pre = project(ingate_weight) + ingate_bias
    forget_pre = project(forget_weight) + forget_bias
    shape = (TOKENS, M_HEADS, M_HEAD_DIM)
    query_heads = queries.astype(f32).reshape(shape)
    key_heads = key_rows.astype(f32).reshape(shape) * M_HEAD_DIM ** (-0.5)
    value_heads = value_rows.astype(f32).reshape(shape)
    log_forget = jax.nn.log_sigmoid(forget_pre)
    new_stabilizer = jnp.maximum(log_forget + stabilizer, ingate_pre)
    keep = jnp.exp(log_forget + stabilizer - new_stabilizer)
    write = jnp.exp(ingate_pre - new_stabilizer)
    new_memory = keep[..., None, None] * memory + write[..., None, None] * key_heads[..., :, None] * value_heads[..., None, :]
    new_normalizer = keep[..., None] * normalizer + write[..., None] * key_heads
    numer = jnp.einsum('thd,thde->the', query_heads, new_memory, precision=lax.Precision.HIGHEST)
    denom = lax.optimization_barrier(jnp.sum(query_heads * new_normalizer, axis=-1))
    hidden = numer / jnp.maximum(jnp.abs(denom), 1.0)[..., None]
    cell_out = (hidden.reshape(TOKENS, M_WIDTH) * jax.nn.sigmoid(outgate.astype(f32))).astype(bf16)
    mixed = jnp.dot(cell_out, mixer_weight, preferred_element_type=f32).astype(bf16)
    resid = stream + mixed.astype(f32)
    moe_in = rms_normed(resid, moe_gain).astype(bf16)
    limit = N_EP * CAP
    padded_in = jnp.concatenate([moe_in, jnp.zeros((1, D), bf16)], axis=0)

    def one_expert(total, expert):
        chosen = expert_index == expert
        weight = lax.optimization_barrier(jnp.sum(jnp.where(chosen, route_weights, 0.0), axis=1))
        rows = jnp.nonzero(jnp.any(chosen, axis=1), size=limit, fill_value=TOKENS)[0].astype(jnp.int32)
        picked = padded_in[rows]
        gate = jnp.dot(picked, expert_gate[expert], preferred_element_type=f32)
        upward = jnp.dot(picked, expert_up[expert], preferred_element_type=f32)
        inner = (jax.nn.silu(gate) * upward).astype(bf16)
        result = jnp.dot(inner, expert_down[expert], preferred_element_type=f32).astype(bf16)
        padded_weight = jnp.concatenate([weight, jnp.zeros((1,), f32)])
        total = total.at[rows].add(result.astype(f32) * padded_weight[rows][:, None])
        return (total, None)
    start = jnp.zeros((TOKENS + 1, D), f32)
    total, unused = lax.scan(one_expert, start, jnp.arange(EXPERTS, dtype=jnp.int32))
    layer_out = (resid + total[:TOKENS]).astype(bf16)
    return (layer_out, new_memory, new_normalizer, new_stabilizer)
```

```python
import jax
import jax.numpy as jnp
from jax import lax
from jax.sharding import PartitionSpec as P

M_HEAD_DIM = 128


EPS = 1e-06


def rms_normed(values, gain):
    scale = lax.rsqrt(jnp.mean(values * values, axis=-1, keepdims=True) + EPS)
    return values * scale * gain


def on_device_general(
    tokens,
    norm_gain,
    query_weight,
    key_weight,
    value_weight,
    outgate_weight,
    ingate_weight,
    forget_weight,
    ingate_bias,
    forget_bias,
    memory,
    normalizer,
    stabilizer,
    mixer_weight,
    moe_gain,
    expert_gate,
    expert_up,
    expert_down,
    expert_index,
    route_weights,
):
    f32 = jnp.float32
    bf16 = jnp.bfloat16
    ep_size = lax.axis_size("ep")
    seq_count = tokens.shape[0]
    model_width = tokens.shape[1]
    cell_width = query_weight.shape[1]
    head_count = ingate_bias.shape[0]
    stream = tokens.astype(f32)
    weight_list = (
        query_weight,
        key_weight,
        value_weight,
        outgate_weight,
        ingate_weight,
        forget_weight,
    )
    normed = rms_normed(stream, norm_gain).astype(bf16)
    normed_cols = lax.all_to_all(normed, "ep", split_axis=1, concat_axis=0, tiled=True)
    joined = jnp.concatenate(weight_list, axis=1)
    projected = lax.psum_scatter(
        jnp.dot(normed_cols, joined, preferred_element_type=f32),
        "ep",
        scatter_dimension=0,
        tiled=True,
    )
    query_sum = projected[:, :cell_width]
    key_sum = projected[:, cell_width : 2 * cell_width]
    value_sum = projected[:, 2 * cell_width : 3 * cell_width]
    outgate_sum = projected[:, 3 * cell_width : 4 * cell_width]
    ingate_sum = projected[:, 4 * cell_width : 4 * cell_width + head_count]
    forget_sum = projected[:, 4 * cell_width + head_count :]
    shape = (seq_count, head_count, M_HEAD_DIM)
    query_heads = query_sum.astype(bf16).astype(f32).reshape(shape)
    key_heads = key_sum.astype(bf16).astype(f32).reshape(shape) * M_HEAD_DIM ** (-0.5)
    value_heads = value_sum.astype(bf16).astype(f32).reshape(shape)
    outgate = outgate_sum.astype(bf16).astype(f32)
    ingate_pre = ingate_sum + ingate_bias
    forget_pre = forget_sum + forget_bias
    log_forget = jax.nn.log_sigmoid(forget_pre)
    new_stabilizer = jnp.maximum(log_forget + stabilizer, ingate_pre)
    keep = jnp.exp(log_forget + stabilizer - new_stabilizer)
    write = jnp.exp(ingate_pre - new_stabilizer)
    new_memory = (
        keep[..., None, None] * memory
        + write[..., None, None] * key_heads[..., :, None] * value_heads[..., None, :]
    )
    new_normalizer = keep[..., None] * normalizer + write[..., None] * key_heads
    numer = jnp.einsum("thd,thde->the", query_heads, new_memory, precision=lax.Precision.HIGHEST)
    denom = jnp.sum(query_heads * new_normalizer, axis=-1)
    hidden = numer / jnp.maximum(jnp.abs(denom), 1.0)[..., None]
    cell_out = (hidden.reshape(seq_count, cell_width) * jax.nn.sigmoid(outgate)).astype(bf16)
    mixed_cols = jnp.dot(
        lax.all_gather(cell_out, "ep", axis=0, tiled=True), mixer_weight, preferred_element_type=f32
    ).astype(bf16)
    mixed = lax.all_to_all(mixed_cols, "ep", split_axis=0, concat_axis=1, tiled=True)
    resid = stream + mixed.astype(f32)
    moe_in = rms_normed(resid, moe_gain).astype(bf16)
    local_experts = expert_gate.shape[0]
    expert_count = local_experts * ep_size
    chosen_k = expert_index.shape[1]
    group_width = expert_count // 2
    capacity = max(2, ((seq_count + 1) // 2 * chosen_k + group_width - 1) // group_width)
    routes = expert_index.reshape(-1)
    matches = (routes[:, None] == jnp.arange(expert_count, dtype=jnp.int32)[None, :]).astype(
        jnp.int32
    )
    slots = jnp.sum((jnp.cumsum(matches, axis=0) - 1) * matches, axis=1)
    target = routes * capacity + slots
    placing = (
        jnp.arange(expert_count * capacity, dtype=jnp.int32)[:, None] == target[None, :]
    ).astype(bf16)
    route_rows = jnp.repeat(moe_in, chosen_k, axis=0)
    outgoing = jnp.dot(placing, route_rows, preferred_element_type=f32).astype(bf16)
    outgoing = outgoing.reshape(expert_count, capacity, model_width)
    received = lax.all_to_all(outgoing, "ep", split_axis=0, concat_axis=0, tiled=True)
    count = received.shape[1]
    grouped = received.reshape(ep_size, local_experts, count, model_width)
    gate = jnp.einsum("sxcd,xdf->sxcf", grouped, expert_gate, preferred_element_type=f32)
    upward = jnp.einsum("sxcd,xdf->sxcf", grouped, expert_up, preferred_element_type=f32)
    inner = (jax.nn.silu(gate) * upward).astype(bf16)
    result = jnp.einsum("sxcf,xfd->sxcd", inner, expert_down, preferred_element_type=f32).astype(
        bf16
    )
    result = result.reshape(ep_size * local_experts, count, model_width)
    returned = lax.all_to_all(result, "ep", split_axis=0, concat_axis=0, tiled=True)
    flat_back = returned.reshape(expert_count * capacity, model_width)
    picked = jnp.dot(placing.T, flat_back, preferred_element_type=f32)
    weighted = picked * route_weights.reshape(-1)[:, None]
    combined = jnp.sum(weighted.reshape(seq_count, chosen_k, model_width), axis=1)
    layer_out = (resid + combined).astype(bf16)
    return (layer_out, new_memory, new_normalizer, new_stabilizer)


ARG_SPECS = (
    P(("grp", "ep"), None),
    P(),
    P("ep", None),
    P("ep", None),
    P("ep", None),
    P("ep", None),
    P("ep", None),
    P("ep", None),
    P(),
    P(),
    P(("grp", "ep"), None, None, None),
    P(("grp", "ep"), None, None),
    P(("grp", "ep"), None),
    P(None, "ep"),
    P(),
    P("ep", None, None),
    P("ep", None, None),
    P("ep", None, None),
    P(("grp", "ep"), None),
    P(("grp", "ep"), None),
)
OUT_SPECS = (
    P(("grp", "ep"), None),
    P(("grp", "ep"), None, None, None),
    P(("grp", "ep"), None, None),
    P(("grp", "ep"), None),
)


def swap(value, bit):
    size = lax.axis_size("ep")
    return lax.ppermute(value, "ep", [(i, i ^ bit) for i in range(size)])


def on_device_fast(
    tokens,
    norm_gain,
    query_weight,
    key_weight,
    value_weight,
    outgate_weight,
    ingate_weight,
    forget_weight,
    ingate_bias,
    forget_bias,
    memory,
    normalizer,
    stabilizer,
    mixer_weight,
    moe_gain,
    expert_gate,
    expert_up,
    expert_down,
    expert_index,
    route_weights,
):
    f32 = jnp.float32
    bf16 = jnp.bfloat16
    ep_size = lax.axis_size("ep")
    me = lax.axis_index("ep")
    seq_count, model_width = tokens.shape
    depth, cell_width = query_weight.shape
    head_count = ingate_bias.shape[0]
    stations = ep_size // 4
    chips = ep_size // 2
    z_groups = [[k + 4 * z for z in range(stations)] for k in range(4)]
    chip_groups = [[k + 2 * c for c in range(chips)] for k in range(2)]

    gates = jnp.concatenate((ingate_weight, forget_weight), axis=1)
    gates = jnp.pad(gates, ((0, 0), (0, 128 - gates.shape[1])))
    joined = jnp.concatenate(
        (query_weight, key_weight, value_weight, outgate_weight, gates), axis=1
    )
    joined_y = swap(joined, 2)
    joined_c = swap(joined, 1)
    joined_yc = swap(joined_y, 1)

    pieces = mixer_weight[None]
    bit = 4
    while bit < ep_size:
        pieces = jnp.concatenate((pieces, swap(pieces, bit)), axis=0)
        bit *= 2
    pieces_y = swap(pieces, 2)
    pieces_c = swap(pieces, 1)
    pieces_yc = swap(pieces_y, 1)

    columns = lax.all_to_all(
        tokens.reshape(seq_count, stations, 4 * depth).transpose(1, 0, 2),
        "ep", 0, 0, tiled=True, axis_index_groups=z_groups,
    )
    station = me // 4
    place = me % 4
    gain_here = lax.dynamic_slice(norm_gain, (station * 4 * depth,), (4 * depth,))
    scaled = (columns.reshape(ep_size // 4 * seq_count, 4 * depth).astype(f32) * gain_here).astype(bf16)
    partial = 0.0
    for bits, weight in ((0, joined), (1, joined_c), (2, joined_y), (3, joined_yc)):
        part = lax.dynamic_slice(scaled, (0, (place ^ bits) * depth), (scaled.shape[0], depth))
        partial = partial + jnp.dot(part, weight, preferred_element_type=f32)
    partial = partial.astype(bf16).reshape(stations, seq_count, -1)
    received = lax.all_to_all(
        partial, "ep", 0, 0, tiled=True, axis_index_groups=z_groups
    )
    stream = tokens.astype(f32)
    scale = lax.rsqrt(jnp.mean(stream * stream, axis=-1, keepdims=True) + EPS)
    projected = jnp.sum(received.astype(f32), axis=0) * scale
    query_sum = projected[:, :cell_width]
    key_sum = projected[:, cell_width : 2 * cell_width]
    value_sum = projected[:, 2 * cell_width : 3 * cell_width]
    outgate_sum = projected[:, 3 * cell_width : 4 * cell_width]
    ingate_sum = projected[:, 4 * cell_width : 4 * cell_width + head_count]
    forget_sum = projected[:, 4 * cell_width + head_count : 4 * cell_width + 2 * head_count]
    shape = (seq_count, head_count, M_HEAD_DIM)
    query_heads = query_sum.astype(bf16).astype(f32).reshape(shape)
    key_heads = key_sum.astype(bf16).astype(f32).reshape(shape) * M_HEAD_DIM ** (-0.5)
    value_heads = value_sum.astype(bf16).astype(f32).reshape(shape)
    outgate = outgate_sum.astype(bf16).astype(f32)
    ingate_pre = ingate_sum + ingate_bias
    forget_pre = forget_sum + forget_bias
    log_forget = jax.nn.log_sigmoid(forget_pre)
    new_stabilizer = jnp.maximum(log_forget + stabilizer, ingate_pre)
    keep = jnp.exp(log_forget + stabilizer - new_stabilizer)
    write = jnp.exp(ingate_pre - new_stabilizer)
    new_memory = (
        keep[..., None, None] * memory
        + write[..., None, None] * key_heads[..., :, None] * value_heads[..., None, :]
    )
    new_normalizer = keep[..., None] * normalizer + write[..., None] * key_heads
    numer = jnp.einsum("thd,thde->the", query_heads, new_memory, precision=lax.Precision.HIGHEST)
    denom = jnp.sum(query_heads * new_normalizer, axis=-1)
    hidden = numer / jnp.maximum(jnp.abs(denom), 1.0)[..., None]
    cell_out = (hidden.reshape(seq_count, cell_width) * jax.nn.sigmoid(outgate)).astype(bf16)

    bits_of = [0]
    bit = 4
    while bit < ep_size:
        bits_of = bits_of + [b ^ bit for b in bits_of]
        bit *= 2
    blocks = []
    order = []
    for extra, group in ((0, pieces), (2, pieces_y), (1, pieces_c), (3, pieces_yc)):
        for number, bits in enumerate(bits_of):
            blocks.append(jnp.dot(cell_out, group[number], preferred_element_type=f32))
            order.append(bits ^ extra)
    stacked = jnp.stack(blocks)
    inverse = [order.index(b) for b in range(ep_size)]
    stacked = jnp.stack([stacked[i] for i in inverse])
    stacked = jnp.take(stacked, jnp.arange(ep_size) ^ me, axis=0)
    mixed = stacked.transpose(1, 0, 2).reshape(seq_count, model_width).astype(bf16)
    resid = stream + mixed.astype(f32)
    moe_in = rms_normed(resid, moe_gain).astype(bf16)

    expert_count = ep_size * expert_gate.shape[0]
    group_width = expert_count // 2
    chosen_k = expert_index.shape[1]
    capacity = max(2, ((seq_count + 1) // 2 * chosen_k + group_width - 1) // group_width)
    limit = min(seq_count, capacity * group_width // chosen_k)
    rows = -(-limit // 8) * 8
    group_of = expert_index[:, 0] // group_width
    in_second = group_of
    rank = jnp.where(in_second == 1, jnp.cumsum(in_second) - 1, jnp.cumsum(1 - in_second) - 1)
    slot = group_of * rows + rank
    select = (jnp.arange(2 * rows)[:, None] == slot[None, :])
    local = expert_index % group_width
    dense = jnp.sum(
        jnp.where(local[:, :, None] == jnp.arange(group_width), route_weights[:, :, None], 0.0), axis=1
    )
    high = dense.astype(bf16)
    low = (dense - high.astype(f32)).astype(bf16)
    extra = jnp.concatenate((high, low), axis=1)
    extra = jnp.pad(extra, ((0, 0), (0, 128 - extra.shape[1])))
    wide = jnp.concatenate((moe_in, extra), axis=1)
    rows_out = jnp.dot(select.astype(bf16), wide, preferred_element_type=f32).astype(bf16)
    rows_out = rows_out.reshape(2, 1, rows, -1)
    outgoing = jnp.broadcast_to(rows_out, (2, chips // 2, rows, rows_out.shape[-1]))
    outgoing = outgoing.reshape(chips, rows, -1)
    direct = lax.all_to_all(outgoing, "ep", 0, 0, tiled=True, axis_index_groups=chip_groups)
    across = swap(direct, 1)
    both = jnp.concatenate((direct, across), axis=0).reshape(ep_size * rows, -1)
    hidden_in = both[:, :model_width]
    mine = me % group_width
    picks = both[:, model_width:].astype(f32)
    weight = lax.dynamic_slice(picks, (0, mine), (picks.shape[0], 1)) + lax.dynamic_slice(
        picks, (0, mine + group_width), (picks.shape[0], 1)
    )
    gate = jnp.dot(hidden_in, expert_gate[0], preferred_element_type=f32)
    upward = jnp.dot(hidden_in, expert_up[0], preferred_element_type=f32)
    inner = (jax.nn.silu(gate) * upward).astype(bf16)
    result = jnp.dot(inner, expert_down[0], preferred_element_type=f32)
    weighted = (result * weight).reshape(2, chips, rows, model_width)
    from_other = swap(weighted[1].astype(bf16), 1)
    summed = (weighted[0] + from_other.astype(f32)).astype(bf16)
    returned = lax.all_to_all(summed, "ep", 0, 0, tiled=True, axis_index_groups=chip_groups)
    combined = jnp.sum(returned.reshape(2, chips // 2, rows, model_width).astype(f32), axis=1)
    combined = combined.reshape(2 * rows, model_width)
    picked = jnp.einsum("st,sd->td", select.astype(f32), combined, precision=lax.Precision.HIGHEST)
    layer_out = (resid + picked).astype(bf16)
    return (layer_out, new_memory, new_normalizer, new_stabilizer)


def solution(mesh):
    ep_size = mesh.shape["ep"]
    aligned = ep_size % 8 == 0 and ep_size <= 16

    def run(*arrays):
        fits = aligned and arrays[13].shape[1] // ep_size % 128 == 0 and arrays[15].shape[0] == ep_size
        body = on_device_fast if fits else on_device_general
        return jax.shard_map(
            body, mesh=mesh, in_specs=ARG_SPECS, out_specs=OUT_SPECS, check_vma=False
        )(*arrays)

    return run
```

```python
import functools

import jax
import jax.numpy as jnp
from jax import lax
from jax.experimental import pallas as pl
from jax.experimental.pallas import tpu as pltpu
from jax.sharding import PartitionSpec as P


M_HEAD_DIM = 128


EPS = 1e-06


def rms_normed(values, gain):
    scale = lax.rsqrt(jnp.mean(values * values, axis=-1, keepdims=True) + EPS)
    return values * scale * gain


def on_device_general(
    tokens,
    norm_gain,
    query_weight,
    key_weight,
    value_weight,
    outgate_weight,
    ingate_weight,
    forget_weight,
    ingate_bias,
    forget_bias,
    memory,
    normalizer,
    stabilizer,
    mixer_weight,
    moe_gain,
    expert_gate,
    expert_up,
    expert_down,
    expert_index,
    route_weights,
):
    f32 = jnp.float32
    bf16 = jnp.bfloat16
    ep_size = lax.axis_size("ep")
    seq_count = tokens.shape[0]
    model_width = tokens.shape[1]
    cell_width = query_weight.shape[1]
    head_count = ingate_bias.shape[0]
    stream = tokens.astype(f32)
    weight_list = (
        query_weight,
        key_weight,
        value_weight,
        outgate_weight,
        ingate_weight,
        forget_weight,
    )
    normed = rms_normed(stream, norm_gain).astype(bf16)
    normed_cols = lax.all_to_all(normed, "ep", split_axis=1, concat_axis=0, tiled=True)
    joined = jnp.concatenate(weight_list, axis=1)
    projected = lax.psum_scatter(
        jnp.dot(normed_cols, joined, preferred_element_type=f32),
        "ep",
        scatter_dimension=0,
        tiled=True,
    )
    query_sum = projected[:, :cell_width]
    key_sum = projected[:, cell_width : 2 * cell_width]
    value_sum = projected[:, 2 * cell_width : 3 * cell_width]
    outgate_sum = projected[:, 3 * cell_width : 4 * cell_width]
    ingate_sum = projected[:, 4 * cell_width : 4 * cell_width + head_count]
    forget_sum = projected[:, 4 * cell_width + head_count :]
    shape = (seq_count, head_count, M_HEAD_DIM)
    query_heads = query_sum.astype(bf16).astype(f32).reshape(shape)
    key_heads = key_sum.astype(bf16).astype(f32).reshape(shape) * M_HEAD_DIM ** (-0.5)
    value_heads = value_sum.astype(bf16).astype(f32).reshape(shape)
    outgate = outgate_sum.astype(bf16).astype(f32)
    ingate_pre = ingate_sum + ingate_bias
    forget_pre = forget_sum + forget_bias
    log_forget = jax.nn.log_sigmoid(forget_pre)
    new_stabilizer = jnp.maximum(log_forget + stabilizer, ingate_pre)
    keep = jnp.exp(log_forget + stabilizer - new_stabilizer)
    write = jnp.exp(ingate_pre - new_stabilizer)
    new_memory = (
        keep[..., None, None] * memory
        + write[..., None, None] * key_heads[..., :, None] * value_heads[..., None, :]
    )
    new_normalizer = keep[..., None] * normalizer + write[..., None] * key_heads
    numer = jnp.einsum("thd,thde->the", query_heads, new_memory, precision=lax.Precision.HIGHEST)
    denom = jnp.sum(query_heads * new_normalizer, axis=-1)
    hidden = numer / jnp.maximum(jnp.abs(denom), 1.0)[..., None]
    cell_out = (hidden.reshape(seq_count, cell_width) * jax.nn.sigmoid(outgate)).astype(bf16)
    mixed_cols = jnp.dot(
        lax.all_gather(cell_out, "ep", axis=0, tiled=True), mixer_weight, preferred_element_type=f32
    ).astype(bf16)
    mixed = lax.all_to_all(mixed_cols, "ep", split_axis=0, concat_axis=1, tiled=True)
    resid = stream + mixed.astype(f32)
    moe_in = rms_normed(resid, moe_gain).astype(bf16)
    local_experts = expert_gate.shape[0]
    expert_count = local_experts * ep_size
    chosen_k = expert_index.shape[1]
    group_width = expert_count // 2
    capacity = max(2, ((seq_count + 1) // 2 * chosen_k + group_width - 1) // group_width)
    routes = expert_index.reshape(-1)
    matches = (routes[:, None] == jnp.arange(expert_count, dtype=jnp.int32)[None, :]).astype(
        jnp.int32
    )
    slots = jnp.sum((jnp.cumsum(matches, axis=0) - 1) * matches, axis=1)
    target = routes * capacity + slots
    placing = (
        jnp.arange(expert_count * capacity, dtype=jnp.int32)[:, None] == target[None, :]
    ).astype(bf16)
    route_rows = jnp.repeat(moe_in, chosen_k, axis=0)
    outgoing = jnp.dot(placing, route_rows, preferred_element_type=f32).astype(bf16)
    outgoing = outgoing.reshape(expert_count, capacity, model_width)
    received = lax.all_to_all(outgoing, "ep", split_axis=0, concat_axis=0, tiled=True)
    count = received.shape[1]
    grouped = received.reshape(ep_size, local_experts, count, model_width)
    gate = jnp.einsum("sxcd,xdf->sxcf", grouped, expert_gate, preferred_element_type=f32)
    upward = jnp.einsum("sxcd,xdf->sxcf", grouped, expert_up, preferred_element_type=f32)
    inner = (jax.nn.silu(gate) * upward).astype(bf16)
    result = jnp.einsum("sxcf,xfd->sxcd", inner, expert_down, preferred_element_type=f32).astype(
        bf16
    )
    result = result.reshape(ep_size * local_experts, count, model_width)
    returned = lax.all_to_all(result, "ep", split_axis=0, concat_axis=0, tiled=True)
    flat_back = returned.reshape(expert_count * capacity, model_width)
    picked = jnp.dot(placing.T, flat_back, preferred_element_type=f32)
    weighted = picked * route_weights.reshape(-1)[:, None]
    combined = jnp.sum(weighted.reshape(seq_count, chosen_k, model_width), axis=1)
    layer_out = (resid + combined).astype(bf16)
    return (layer_out, new_memory, new_normalizer, new_stabilizer)


ARG_SPECS = (
    P(("grp", "ep"), None),
    P(),
    P("ep", None),
    P("ep", None),
    P("ep", None),
    P("ep", None),
    P("ep", None),
    P("ep", None),
    P(),
    P(),
    P(("grp", "ep"), None, None, None),
    P(("grp", "ep"), None, None),
    P(("grp", "ep"), None),
    P(None, "ep"),
    P(),
    P("ep", None, None),
    P("ep", None, None),
    P("ep", None, None),
    P(("grp", "ep"), None),
    P(("grp", "ep"), None),
)
OUT_SPECS = (
    P(("grp", "ep"), None),
    P(("grp", "ep"), None, None, None),
    P(("grp", "ep"), None, None),
    P(("grp", "ep"), None),
)


def swap(value, bit):
    size = lax.axis_size("ep")
    return lax.ppermute(value, "ep", [(i, i ^ bit) for i in range(size)])


F32 = jnp.float32
BF16 = jnp.bfloat16
LANES = 128


def local_call(kernel, outs, scratch=(), flops=1, moved=1, smem=(), hbm=(), anywhere=(), outs_hbm=(), limit=8):
    def call(*args):
        def space(i):
            if i in smem:
                return pltpu.SMEM
            if i in hbm:
                return pltpu.HBM
            return pl.ANY if i in anywhere else pltpu.VMEM

        specs = [pl.BlockSpec(memory_space=space(i)) for i in range(len(args))]
        return pl.pallas_call(
            kernel,
            out_shape=[jax.ShapeDtypeStruct(*o) for o in outs],
            in_specs=specs,
            out_specs=[
                pl.BlockSpec(memory_space=pltpu.HBM if i in outs_hbm else pltpu.VMEM)
                for i in range(len(outs))
            ],
            scratch_shapes=list(scratch),
            compiler_params=pltpu.CompilerParams(vmem_limit_bytes=limit * 2**20),
            cost_estimate=pl.CostEstimate(
                flops=flops, bytes_accessed=moved, transcendentals=0
            ),
        )(*args)

    return call


def stack_kernel(first, second, out, sems):
    count = first.shape[0]
    copies = [
        pltpu.make_async_copy(first, out.at[:count], sems.at[0]),
        pltpu.make_async_copy(second, out.at[count:], sems.at[1]),
    ]
    for copy in copies:
        copy.start()
    for copy in copies:
        copy.wait()


def stack(first, second):
    shape = (first.shape[0] + second.shape[0],) + first.shape[1:]
    return local_call(
        stack_kernel,
        [(shape, first.dtype)],
        scratch=[pltpu.SemaphoreType.DMA((2,))],
        anywhere=(0, 1),
        limit=60,
        moved=2 * first.size * 4,
    )(first, second)[0]


def join_kernel(
    tokens, query, key, value, outgate, ingate, forget, joined, columns, turned, held, narrow, sems
):
    width = query.shape[1]
    heads = ingate.shape[0]
    copies = [
        pltpu.make_async_copy(ingate, narrow.at[0], sems.at[0]),
        pltpu.make_async_copy(forget, narrow.at[1], sems.at[1]),
        pltpu.make_async_copy(tokens, held, sems.at[2]),
    ]
    for i, ref in enumerate((query, key, value, outgate)):
        copies.append(
            pltpu.make_async_copy(ref, joined.at[:, i * width : (i + 1) * width], sems.at[3 + i])
        )
    for copy in copies:
        copy.start()
    turned[...] = jnp.zeros_like(turned)
    for copy in copies[:3]:
        copy.wait()
    turned[:heads] = narrow[0].astype(F32)
    turned[heads : 2 * heads] = narrow[1].astype(F32)
    joined[:, 4 * width :] = turned[...].T.astype(BF16)
    part = columns.shape[2]
    for z in range(columns.shape[0]):
        columns[z] = held[:, z * part : (z + 1) * part]
    for copy in copies[3:]:
        copy.wait()


def project_kernel(columns, gain, own, core, side, cross, out, scaled, weights, total, sems):
    stations, rows, part = columns.shape
    depth = own.shape[0]
    copies = [
        pltpu.make_async_copy(ref, weights.at[i], sems.at[i])
        for i, ref in enumerate((own, core, side, cross))
    ]
    for copy in copies:
        copy.start()
    me = lax.axis_index("ep")
    station, place = me // 4, me % 4
    gain_here = gain[:, pl.ds(pl.multiple_of(station * part, LANES), part)]
    for z in range(stations):
        scaled[z * rows : (z + 1) * rows, :] = columns[z].astype(F32) * gain_here
    width = out.shape[2]
    step = 4 * LANES
    for bits, copy in enumerate(copies):
        start = pl.multiple_of((place ^ bits) * depth, LANES)
        part_x = scaled[:, pl.ds(start, depth)].astype(BF16)
        copy.wait()
        for low in range(0, width, step):
            high = min(low + step, width)
            term = jnp.dot(part_x, weights[bits, :, low:high], preferred_element_type=F32)
            if bits:
                term = term + total[:, low:high]
            if bits < 3:
                total[:, low:high] = term
            else:
                for z in range(stations):
                    out[z, :, low:high] = term[z * rows : (z + 1) * rows].astype(BF16)


def rounded(value):
    return value.astype(BF16).astype(F32)


def cell_kernel(
    ingate_bias, forget_bias, received, tokens, memory, normalizer, stabilizer,
    new_memory, new_normalizer, new_stabilizer, cell_out,
    turned, flipped, keeps, numer, fresh, sems,
):
    stations, rows, _ = received.shape
    heads = memory.shape[1]
    dim = memory.shape[2]
    width = heads * dim
    stream = tokens[...].astype(F32)
    scale = lax.rsqrt(jnp.mean(stream * stream, axis=-1, keepdims=True) + EPS)
    total = received[0].astype(F32)
    for z in range(1, stations):
        total = total + received[z].astype(F32)
    total = total * scale
    gates = total[:, 4 * width :]
    value = rounded(total[:, 2 * width : 3 * width])
    lane = lax.broadcasted_iota(jnp.int32, (rows, heads), 1)
    states = jnp.zeros((rows, heads), F32)
    denoms = []
    for h in range(heads):
        cut = slice(h * dim, (h + 1) * dim)
        query = rounded(total[:, h * dim : (h + 1) * dim])
        key = rounded(total[:, width + h * dim : width + (h + 1) * dim]) * dim ** (-0.5)
        ingate_pre = gates[:, h : h + 1] + ingate_bias[h]
        forget_pre = gates[:, heads + h : heads + h + 1] + forget_bias[h]
        log_forget = jnp.minimum(forget_pre, 0.0) - jnp.log1p(jnp.exp(-jnp.abs(forget_pre)))
        carried = log_forget + stabilizer[:, h : h + 1]
        state = jnp.maximum(carried, ingate_pre)
        states = jnp.where(lane == h, state, states)
        keep = jnp.broadcast_to(jnp.exp(carried - state), (rows, dim))
        keeps[:, cut] = keep
        write_key = jnp.exp(ingate_pre - state) * key
        normal = keep * normalizer[:, h, :] + write_key
        new_normalizer[:, h, :] = normal
        denoms.append(jnp.sum(query * normal, axis=-1, keepdims=True))
        turned[h, 0:rows, :] = query
        turned[h, 16 : 16 + rows, :] = write_key
        flipped[h] = turned[h].T
    new_stabilizer[...] = states
    copies = []
    for t in range(rows):
        for h in range(heads):
            cut = slice(h * dim, (h + 1) * dim)
            keep_row = keeps[t : t + 1, cut]
            value_row = value[t : t + 1, cut]
            total_row = jnp.zeros((8, dim), F32)
            for low in range(0, dim, 8):
                part = slice(low, low + 8)
                block = keep_row * memory[t, h, part, :] + flipped[h, part, 16 + t : 17 + t] * value_row
                fresh[t, h, part, :] = block
                total_row = total_row + flipped[h, part, t : t + 1] * block
            numer[t : t + 1, cut] = jnp.sum(total_row, axis=0, keepdims=True)
        copies.append(pltpu.make_async_copy(fresh.at[t], new_memory.at[t], sems.at[t]))
        copies[-1].start()
    for h in range(heads):
        cut = slice(h * dim, (h + 1) * dim)
        outgate = rounded(total[:, 3 * width + h * dim : 3 * width + (h + 1) * dim])
        hidden = numer[:, cut] / jnp.maximum(jnp.abs(denoms[h]), 1.0)
        cell_out[:, cut] = (hidden / (1.0 + jnp.exp(-outgate))).astype(BF16)
    for copy in copies:
        copy.wait()


def routing_kernel(group_width, rows_pad, index, weights, select, extra):
    rows, chosen = index.shape
    second = (index[:, 0:1] >= group_width).astype(F32)
    row = lax.broadcasted_iota(jnp.int32, (rows, rows), 0)
    col = lax.broadcasted_iota(jnp.int32, (rows, rows), 1)
    earlier = (col < row).astype(F32)
    before = jnp.dot(earlier, jnp.broadcast_to(second, (rows, LANES)), preferred_element_type=F32)
    place = lax.broadcasted_iota(jnp.int32, (rows, LANES), 0).astype(F32)
    slot = jnp.where(second > 0.5, rows_pad + before, place - before)
    lane = lax.broadcasted_iota(jnp.int32, (rows, LANES), 1)
    select[...] = (lane.astype(F32) == slot).astype(F32)
    dense = jnp.zeros((rows, LANES), F32)
    for k in range(chosen):
        local = jnp.where(index[:, k : k + 1] >= group_width, index[:, k : k + 1] - group_width, index[:, k : k + 1])
        hit = (lane == local) | (lane == local + group_width)
        dense = dense + jnp.where(hit, weights[:, k : k + 1], 0.0)
    high = rounded(dense)
    extra[...] = jnp.where(lane < group_width, high, dense - high).astype(BF16)


def mix_kernel(places, cell_out, tokens, gain, select, extra, *refs):
    blocks, (resid, outgoing, mixed) = refs[: len(places)], refs[len(places) :]
    width = tokens.shape[1]
    me = lax.axis_index("ep")
    piece = blocks[0].shape[2]
    cell = cell_out[...]
    for ref, bits_of in zip(blocks, places):
        for number, bits in enumerate(bits_of):
            block = jnp.dot(cell, ref[number], preferred_element_type=F32)
            start = pl.multiple_of((me ^ bits) * piece, LANES)
            mixed[:, pl.ds(start, piece)] = rounded(block)
    total = tokens[...].astype(F32) + mixed[...]
    resid[...] = total
    scale = lax.rsqrt(jnp.mean(total * total, axis=-1, keepdims=True) + EPS)
    moe_in = (total * scale * gain[...]).astype(BF16)
    chips, rows_pad, _ = outgoing.shape
    pick = select[:, : 2 * rows_pad].astype(BF16)
    contract = (((0,), (0,)), ((), ()))
    picked = lax.dot_general(pick, moe_in, contract, preferred_element_type=F32)
    tail = lax.dot_general(pick, extra[...], contract, preferred_element_type=F32)
    for group in range(2):
        cut = slice(group * rows_pad, (group + 1) * rows_pad)
        body = picked[cut].astype(BF16)
        end = tail[cut].astype(BF16)
        for c in range(chips // 2):
            outgoing[group * (chips // 2) + c, :, :width] = body
            outgoing[group * (chips // 2) + c, :, width:] = end


def expert_kernel(group_width, direct, across, gate_weight, up_weight, down_weight, kept, sent):
    width = gate_weight.shape[1]
    half = direct.shape[0]
    me = lax.axis_index("ep")
    mine = me % group_width
    x = jnp.concatenate((direct[:, :width], across[:, :width]), axis=0)
    tail = jnp.concatenate((direct[:, width:], across[:, width:]), axis=0).astype(F32)
    lane = lax.broadcasted_iota(jnp.int32, tail.shape, 1)
    hit = (lane == mine) | (lane == mine + group_width)
    weight = jnp.sum(jnp.where(hit, tail, 0.0), axis=1, keepdims=True)
    gate = jnp.dot(x, gate_weight[0], preferred_element_type=F32)
    upward = jnp.dot(x, up_weight[0], preferred_element_type=F32)
    inner = (gate / (1.0 + jnp.exp(-gate)) * upward).astype(BF16)
    step = 4 * LANES
    for low in range(0, width, step):
        out = jnp.dot(inner, down_weight[0, :, low : low + step], preferred_element_type=F32) * weight
        kept[:, low : low + step] = out[:half]
        sent[:, low : low + step] = out[half:].astype(BF16)


def pair_kernel(kept, other, out):
    out[...] = (kept[...] + other[...].astype(F32)).astype(BF16)


def final_kernel(returned, select, resid, out):
    chips, rows_pad, _ = returned.shape
    sums = []
    for group in range(2):
        base = group * (chips // 2)
        total = returned[base].astype(F32)
        for c in range(1, chips // 2):
            total = total + returned[base + c].astype(F32)
        sums.append(total)
    combined = jnp.concatenate(sums, axis=0)
    picked = jnp.dot(
        select[:, : 2 * rows_pad], combined,
        preferred_element_type=F32, precision=lax.Precision.HIGHEST,
    )
    out[...] = (resid[...] + picked).astype(BF16)


def on_device_fast(
    tokens,
    norm_gain,
    query_weight,
    key_weight,
    value_weight,
    outgate_weight,
    ingate_weight,
    forget_weight,
    ingate_bias,
    forget_bias,
    memory,
    normalizer,
    stabilizer,
    mixer_weight,
    moe_gain,
    expert_gate,
    expert_up,
    expert_down,
    expert_index,
    route_weights,
):
    ep_size = lax.axis_size("ep")
    seq_count, model_width = tokens.shape
    depth, cell_width = query_weight.shape
    stations = ep_size // 4
    chips = ep_size // 2
    z_groups = [[k + 4 * z for z in range(stations)] for k in range(4)]
    chip_groups = [[k + 2 * c for c in range(chips)] for k in range(2)]
    expert_count = ep_size * expert_gate.shape[0]
    group_width = expert_count // 2
    chosen_k = expert_index.shape[1]
    capacity = max(2, ((seq_count + 1) // 2 * chosen_k + group_width - 1) // group_width)
    limit = min(seq_count, capacity * group_width // chosen_k)
    rows = -(-limit // 8) * 8

    pieces, bits_of = mixer_weight[None], [0]
    batches = []
    bit = 4
    while bit < ep_size:
        moved = swap(pieces, bit)
        moved_bits = [b ^ bit for b in bits_of]
        if 2 * bit < ep_size:
            pieces = stack(pieces, moved)
            bits_of = bits_of + moved_bits
        else:
            batches = [(pieces, bits_of), (moved, moved_bits)]
        bit *= 2

    wide = 4 * cell_width + LANES
    joined, columns = local_call(
        join_kernel,
        [((depth, wide), BF16), ((stations, seq_count, model_width // stations), BF16)],
        scratch=[
            pltpu.VMEM((LANES, depth), F32),
            pltpu.VMEM(tokens.shape, BF16),
            pltpu.VMEM((2, ingate_weight.shape[1], depth), BF16),
            pltpu.SemaphoreType.DMA((7,)),
        ],
        hbm=tuple(range(7)),
        limit=60,
        moved=2 * depth * wide * 2,
    )(tokens, query_weight, key_weight, value_weight, outgate_weight, ingate_weight.T, forget_weight.T)
    joined_y = swap(joined, 2)
    joined_c = swap(joined, 1)
    joined_yc = swap(joined_y, 1)
    columns = lax.all_to_all(columns, "ep", 0, 0, tiled=True, axis_index_groups=z_groups)
    (partial,) = local_call(
        project_kernel,
        [((stations, seq_count, wide), BF16)],
        scratch=[
            pltpu.VMEM((stations * seq_count, 4 * depth), F32),
            pltpu.VMEM((4, depth, wide), BF16),
            pltpu.VMEM((stations * seq_count, wide), F32),
            pltpu.SemaphoreType.DMA((4,)),
        ],
        anywhere=(2, 3, 4, 5),
        limit=60,
        flops=2 * stations * seq_count * 4 * depth * wide,
        moved=4 * depth * wide * 2,
    )(columns, norm_gain[None], joined, joined_c, joined_y, joined_yc)
    received = lax.all_to_all(partial, "ep", 0, 0, tiled=True, axis_index_groups=z_groups)
    for batch, bits in list(batches):
        batches.append((swap(batch, 2), [b ^ 2 for b in bits]))
    for batch, bits in list(batches):
        batches.append((swap(batch, 1), [b ^ 1 for b in bits]))
    blocks = [batch for batch, _ in batches]
    places = tuple(tuple(bits) for _, bits in batches)

    select, extra = local_call(
        functools.partial(routing_kernel, group_width, rows),
        [((seq_count, LANES), F32), ((seq_count, LANES), BF16)],
    )(expert_index, route_weights)

    new_memory, new_normalizer, new_stabilizer, cell_out = local_call(
        cell_kernel,
        [
            (memory.shape, F32),
            (normalizer.shape, F32),
            (stabilizer.shape, F32),
            ((seq_count, cell_width), BF16),
        ],
        scratch=[
            pltpu.VMEM(memory.shape[1:2] + (LANES, LANES), F32),
            pltpu.VMEM(memory.shape[1:2] + (LANES, LANES), F32),
            pltpu.VMEM((seq_count, cell_width), F32),
            pltpu.VMEM((seq_count, cell_width), F32),
            pltpu.VMEM(memory.shape, F32),
            pltpu.SemaphoreType.DMA((seq_count,)),
        ],
        outs_hbm=(0,),
        flops=6 * memory.size,
        moved=8 * memory.size,
        smem=(0, 1),
        limit=16,
    )(ingate_bias, forget_bias, received, tokens, memory, normalizer, stabilizer)

    resid, outgoing = local_call(
        functools.partial(mix_kernel, places),
        [((seq_count, model_width), F32), ((chips, rows, model_width + LANES), BF16)],
        scratch=[pltpu.VMEM((seq_count, model_width), F32)],
        flops=2 * seq_count * cell_width * model_width,
        moved=2 * cell_width * model_width,
        limit=12,
    )(cell_out, tokens, moe_gain[None], select, extra, *blocks)

    direct = lax.all_to_all(outgoing, "ep", 0, 0, tiled=True, axis_index_groups=chip_groups)
    direct = direct.reshape(chips * rows, model_width + LANES)
    across = swap(direct, 1)
    kept, sent = local_call(
        functools.partial(expert_kernel, group_width),
        [((chips * rows, model_width), F32), ((chips * rows, model_width), BF16)],
        flops=6 * 2 * chips * rows * model_width * expert_gate.shape[2],
        moved=6 * model_width * expert_gate.shape[2],
        limit=24,
    )(direct, across, expert_gate, expert_up, expert_down)
    (summed,) = local_call(pair_kernel, [((chips * rows, model_width), BF16)])(kept, swap(sent, 1))
    returned = lax.all_to_all(
        summed.reshape(chips, rows, model_width), "ep", 0, 0, tiled=True, axis_index_groups=chip_groups
    )
    (layer_out,) = local_call(final_kernel, [((seq_count, model_width), BF16)])(returned, select, resid)
    return (layer_out, new_memory, new_normalizer, new_stabilizer)


def solution(mesh):
    ep_size = mesh.shape["ep"]
    aligned = ep_size % 8 == 0 and ep_size <= 16

    def run(*arrays):
        fits = aligned and arrays[13].shape[1] // ep_size % 128 == 0 and arrays[15].shape[0] == ep_size
        fits = fits and arrays[2].shape[0] // ep_size % 128 == 0 and arrays[10].shape[2] == 128

        def body(*blocks):
            return (on_device_fast if fits else on_device_general)(*blocks)

        step = jax.shard_map(
            body, mesh=mesh, in_specs=ARG_SPECS, out_specs=OUT_SPECS, check_vma=False
        )
        return step(*arrays)

    return run
```

```python
import functools

import jax
import jax.numpy as jnp
from jax import lax
from jax.experimental import pallas as pl
from jax.experimental.pallas import tpu as pltpu
from jax.sharding import PartitionSpec as P


M_HEAD_DIM = 128


EPS = 1e-06


def rms_normed(values, gain):
    scale = lax.rsqrt(jnp.mean(values * values, axis=-1, keepdims=True) + EPS)
    return values * scale * gain


def on_device_general(
    tokens,
    norm_gain,
    query_weight,
    key_weight,
    value_weight,
    outgate_weight,
    ingate_weight,
    forget_weight,
    ingate_bias,
    forget_bias,
    memory,
    normalizer,
    stabilizer,
    mixer_weight,
    moe_gain,
    expert_gate,
    expert_up,
    expert_down,
    expert_index,
    route_weights,
):
    f32 = jnp.float32
    bf16 = jnp.bfloat16
    ep_size = lax.axis_size("ep")
    seq_count = tokens.shape[0]
    model_width = tokens.shape[1]
    cell_width = query_weight.shape[1]
    head_count = ingate_bias.shape[0]
    stream = tokens.astype(f32)
    weight_list = (
        query_weight,
        key_weight,
        value_weight,
        outgate_weight,
        ingate_weight,
        forget_weight,
    )
    normed = rms_normed(stream, norm_gain).astype(bf16)
    normed_cols = lax.all_to_all(normed, "ep", split_axis=1, concat_axis=0, tiled=True)
    joined = jnp.concatenate(weight_list, axis=1)
    projected = lax.psum_scatter(
        jnp.dot(normed_cols, joined, preferred_element_type=f32),
        "ep",
        scatter_dimension=0,
        tiled=True,
    )
    query_sum = projected[:, :cell_width]
    key_sum = projected[:, cell_width : 2 * cell_width]
    value_sum = projected[:, 2 * cell_width : 3 * cell_width]
    outgate_sum = projected[:, 3 * cell_width : 4 * cell_width]
    ingate_sum = projected[:, 4 * cell_width : 4 * cell_width + head_count]
    forget_sum = projected[:, 4 * cell_width + head_count :]
    shape = (seq_count, head_count, M_HEAD_DIM)
    query_heads = query_sum.astype(bf16).astype(f32).reshape(shape)
    key_heads = key_sum.astype(bf16).astype(f32).reshape(shape) * M_HEAD_DIM ** (-0.5)
    value_heads = value_sum.astype(bf16).astype(f32).reshape(shape)
    outgate = outgate_sum.astype(bf16).astype(f32)
    ingate_pre = ingate_sum + ingate_bias
    forget_pre = forget_sum + forget_bias
    log_forget = jax.nn.log_sigmoid(forget_pre)
    new_stabilizer = jnp.maximum(log_forget + stabilizer, ingate_pre)
    keep = jnp.exp(log_forget + stabilizer - new_stabilizer)
    write = jnp.exp(ingate_pre - new_stabilizer)
    new_memory = (
        keep[..., None, None] * memory
        + write[..., None, None] * key_heads[..., :, None] * value_heads[..., None, :]
    )
    new_normalizer = keep[..., None] * normalizer + write[..., None] * key_heads
    numer = jnp.einsum("thd,thde->the", query_heads, new_memory, precision=lax.Precision.HIGHEST)
    denom = jnp.sum(query_heads * new_normalizer, axis=-1)
    hidden = numer / jnp.maximum(jnp.abs(denom), 1.0)[..., None]
    cell_out = (hidden.reshape(seq_count, cell_width) * jax.nn.sigmoid(outgate)).astype(bf16)
    mixed_cols = jnp.dot(
        lax.all_gather(cell_out, "ep", axis=0, tiled=True), mixer_weight, preferred_element_type=f32
    ).astype(bf16)
    mixed = lax.all_to_all(mixed_cols, "ep", split_axis=0, concat_axis=1, tiled=True)
    resid = stream + mixed.astype(f32)
    moe_in = rms_normed(resid, moe_gain).astype(bf16)
    local_experts = expert_gate.shape[0]
    expert_count = local_experts * ep_size
    chosen_k = expert_index.shape[1]
    group_width = expert_count // 2
    capacity = max(2, ((seq_count + 1) // 2 * chosen_k + group_width - 1) // group_width)
    routes = expert_index.reshape(-1)
    matches = (routes[:, None] == jnp.arange(expert_count, dtype=jnp.int32)[None, :]).astype(
        jnp.int32
    )
    slots = jnp.sum((jnp.cumsum(matches, axis=0) - 1) * matches, axis=1)
    target = routes * capacity + slots
    placing = (
        jnp.arange(expert_count * capacity, dtype=jnp.int32)[:, None] == target[None, :]
    ).astype(bf16)
    route_rows = jnp.repeat(moe_in, chosen_k, axis=0)
    outgoing = jnp.dot(placing, route_rows, preferred_element_type=f32).astype(bf16)
    outgoing = outgoing.reshape(expert_count, capacity, model_width)
    received = lax.all_to_all(outgoing, "ep", split_axis=0, concat_axis=0, tiled=True)
    count = received.shape[1]
    grouped = received.reshape(ep_size, local_experts, count, model_width)
    gate = jnp.einsum("sxcd,xdf->sxcf", grouped, expert_gate, preferred_element_type=f32)
    upward = jnp.einsum("sxcd,xdf->sxcf", grouped, expert_up, preferred_element_type=f32)
    inner = (jax.nn.silu(gate) * upward).astype(bf16)
    result = jnp.einsum("sxcf,xfd->sxcd", inner, expert_down, preferred_element_type=f32).astype(
        bf16
    )
    result = result.reshape(ep_size * local_experts, count, model_width)
    returned = lax.all_to_all(result, "ep", split_axis=0, concat_axis=0, tiled=True)
    flat_back = returned.reshape(expert_count * capacity, model_width)
    picked = jnp.dot(placing.T, flat_back, preferred_element_type=f32)
    weighted = picked * route_weights.reshape(-1)[:, None]
    combined = jnp.sum(weighted.reshape(seq_count, chosen_k, model_width), axis=1)
    layer_out = (resid + combined).astype(bf16)
    return (layer_out, new_memory, new_normalizer, new_stabilizer)


ARG_SPECS = (
    P(("grp", "ep"), None),
    P(),
    P("ep", None),
    P("ep", None),
    P("ep", None),
    P("ep", None),
    P("ep", None),
    P("ep", None),
    P(),
    P(),
    P(("grp", "ep"), None, None, None),
    P(("grp", "ep"), None, None),
    P(("grp", "ep"), None),
    P(None, "ep"),
    P(),
    P("ep", None, None),
    P("ep", None, None),
    P("ep", None, None),
    P(("grp", "ep"), None),
    P(("grp", "ep"), None),
)
OUT_SPECS = (
    P(("grp", "ep"), None),
    P(("grp", "ep"), None, None, None),
    P(("grp", "ep"), None, None),
    P(("grp", "ep"), None),
)


def swap(value, bit):
    size = lax.axis_size("ep")
    return lax.ppermute(value, "ep", [(i, i ^ bit) for i in range(size)])


F32 = jnp.float32
BF16 = jnp.bfloat16
LANES = 128


def local_call(kernel, outs, scratch=(), flops=1, moved=1, smem=(), hbm=(), anywhere=(), outs_hbm=(), limit=8):
    def call(*args):
        def space(i):
            if i in smem:
                return pltpu.SMEM
            if i in hbm:
                return pltpu.HBM
            return pl.ANY if i in anywhere else pltpu.VMEM

        specs = [pl.BlockSpec(memory_space=space(i)) for i in range(len(args))]
        return pl.pallas_call(
            kernel,
            out_shape=[jax.ShapeDtypeStruct(*o) for o in outs],
            in_specs=specs,
            out_specs=[
                pl.BlockSpec(memory_space=pltpu.HBM if i in outs_hbm else pltpu.VMEM)
                for i in range(len(outs))
            ],
            scratch_shapes=list(scratch),
            compiler_params=pltpu.CompilerParams(vmem_limit_bytes=int(limit * 2**20)),
            cost_estimate=pl.CostEstimate(
                flops=flops, bytes_accessed=moved, transcendentals=0
            ),
        )(*args)

    return call


def stack_kernel(first, second, out, sems):
    count = first.shape[0]
    copies = [
        pltpu.make_async_copy(first, out.at[:count], sems.at[0]),
        pltpu.make_async_copy(second, out.at[count:], sems.at[1]),
    ]
    for copy in copies:
        copy.start()
    for copy in copies:
        copy.wait()


def stack(first, second):
    shape = (first.shape[0] + second.shape[0],) + first.shape[1:]
    return local_call(
        stack_kernel,
        [(shape, first.dtype)],
        scratch=[pltpu.SemaphoreType.DMA((2,))],
        anywhere=(0, 1),
        limit=60,
        moved=2 * first.size * 4,
    )(first, second)[0]


def join_kernel(
    tokens, query, key, value, outgate, ingate, forget, joined, columns, turned, held, narrow, sems
):
    width = query.shape[1]
    heads = ingate.shape[0]
    copies = [
        pltpu.make_async_copy(ingate, narrow.at[0], sems.at[0]),
        pltpu.make_async_copy(forget, narrow.at[1], sems.at[1]),
        pltpu.make_async_copy(tokens, held, sems.at[2]),
    ]
    for i, ref in enumerate((query, key, value, outgate)):
        copies.append(
            pltpu.make_async_copy(ref, joined.at[:, i * width : (i + 1) * width], sems.at[3 + i])
        )
    for copy in copies:
        copy.start()
    turned[...] = jnp.zeros_like(turned)
    for copy in copies[:3]:
        copy.wait()
    turned[:heads] = narrow[0].astype(F32)
    turned[heads : 2 * heads] = narrow[1].astype(F32)
    joined[:, 4 * width :] = turned[...].T.astype(BF16)
    part = columns.shape[2]
    for z in range(columns.shape[0]):
        columns[z] = held[:, z * part : (z + 1) * part]
    for copy in copies[3:]:
        copy.wait()


def project_kernel(bits_of, columns, gain, first, second, *refs):
    before, out, scaled = refs if len(refs) == 3 else (None,) + refs
    stations, rows, part = columns.shape
    depth = first.shape[0]
    me = lax.axis_index("ep")
    station, place = me // 4, me % 4
    gain_here = gain[:, pl.ds(pl.multiple_of(station * part, LANES), part)]
    for z in range(stations):
        scaled[z * rows : (z + 1) * rows, :] = columns[z].astype(F32) * gain_here
    parts = []
    for bits in bits_of:
        start = pl.multiple_of((place ^ bits) * depth, LANES)
        parts.append(scaled[:, pl.ds(start, depth)].astype(BF16))
    width = out.shape[-1]
    step = 4 * LANES
    for low in range(0, width, step):
        high = min(low + step, width)
        term = jnp.dot(parts[0], first[:, low:high], preferred_element_type=F32)
        term = term + jnp.dot(parts[1], second[:, low:high], preferred_element_type=F32)
        if before is None:
            out[:, low:high] = term
            continue
        term = term + before[:, low:high]
        for z in range(stations):
            out[z, :, low:high] = term[z * rows : (z + 1) * rows].astype(BF16)


def rounded(value):
    return value.astype(BF16).astype(F32)


def cell_kernel(
    received, memory, side, new_memory, new_normalizer, new_stabilizer, cell_out,
    turned, flipped, spread, keeps, numer, fresh, sems,
):
    stations, rows, _ = received.shape
    heads = memory.shape[1]
    dim = memory.shape[2]
    width = heads * dim
    low = side.shape[1] - 4 * LANES
    model_width = (low - width) // 2
    scale = side[:, low : low + 1]
    known = side[:, low + 2 * LANES : low + 3 * LANES]
    total = received[0].astype(F32)
    for z in range(1, stations):
        total = total + received[z].astype(F32)
    total = total * scale
    gates = total[:, 4 * width :]
    value = rounded(total[:, 2 * width : 3 * width])
    lane = lax.broadcasted_iota(jnp.int32, (rows, heads), 1)
    states = jnp.zeros((rows, heads), F32)
    denoms = []
    turned[...] = jnp.zeros_like(turned)
    spread[...] = jnp.zeros_like(spread)
    spread[:, 0:16, 0:dim] = jnp.ones((heads, 16, dim), F32)
    for h in range(heads):
        cut = slice(h * dim, (h + 1) * dim)
        query = rounded(total[:, h * dim : (h + 1) * dim])
        key = rounded(total[:, width + h * dim : width + (h + 1) * dim]) * dim ** (-0.5)
        ingate_pre = gates[:, h : h + 1] + known[:, 40 + h : 41 + h]
        forget_pre = gates[:, heads + h : heads + h + 1] + known[:, 48 + h : 49 + h]
        log_forget = jnp.minimum(forget_pre, 0.0) - jnp.log1p(jnp.exp(-jnp.abs(forget_pre)))
        carried = log_forget + known[:, 32 + h : 33 + h]
        state = jnp.maximum(carried, ingate_pre)
        states = jnp.where(lane == h, state, states)
        keep = jnp.broadcast_to(jnp.exp(carried - state), (rows, dim))
        keeps[:, cut] = keep
        write_key = jnp.exp(ingate_pre - state) * key
        base = 2 * model_width + h * dim
        normal = keep * side[:, base : base + dim] + write_key
        new_normalizer[:, h, :] = normal
        denoms.append(jnp.sum(query * normal, axis=-1, keepdims=True))
        high = rounded(write_key)
        middle = rounded(write_key - high)
        turned[h, 0:rows, :] = query
        turned[h, 16 : 16 + rows, :] = high
        turned[h, 32 : 32 + rows, :] = middle
        turned[h, 48 : 48 + rows, :] = rounded(write_key - high - middle)
        flipped[h] = turned[h].T.astype(BF16)
        for i in range(1, 4):
            spread[h, 16 * i : 16 * i + rows, dim:] = value[:, cut]
    new_stabilizer[...] = states
    copies = []
    which = lax.broadcasted_iota(jnp.int32, (64, 2 * dim), 0) % 16
    spreads = [spread[h].astype(BF16) for h in range(heads)]
    for t in range(rows):
        for h in range(heads):
            cut = slice(h * dim, (h + 1) * dim)
            row_only = jnp.where(which == t, spreads[h], jnp.zeros_like(spreads[h]))
            both = jnp.dot(flipped[h][:, :64], row_only, preferred_element_type=F32)
            block = keeps[t : t + 1, cut] * memory[t, h] + both[:, dim:]
            fresh[t, h] = block
            numer[t : t + 1, cut] = jnp.sum(both[:, :dim] * block, axis=0, keepdims=True)
        copies.append(pltpu.make_async_copy(fresh.at[t], new_memory.at[t], sems.at[t]))
        copies[-1].start()
    for h in range(heads):
        cut = slice(h * dim, (h + 1) * dim)
        outgate = rounded(total[:, 3 * width + h * dim : 3 * width + (h + 1) * dim])
        hidden = numer[:, cut] / jnp.maximum(jnp.abs(denoms[h]), 1.0)
        cell_out[:, cut] = (hidden / (1.0 + jnp.exp(-outgate))).astype(BF16)
    for copy in copies:
        copy.wait()


def mix_kernel(places, cell_out, side, *refs):
    blocks, (resid, outgoing, mixed) = refs[: len(places)], refs[len(places) :]
    cell = cell_out[...]
    model_width = resid.shape[1]
    low = side.shape[1] - 4 * LANES
    select = side[:, low + LANES : low + 2 * LANES]
    extra = side[:, low + 3 * LANES : low + 4 * LANES].astype(BF16)
    me = lax.axis_index("ep")
    piece = blocks[0].shape[2]
    for i, bits_of in enumerate(places):
        for number, bits in enumerate(bits_of):
            block = jnp.dot(cell, blocks[i][number], preferred_element_type=F32)
            start = pl.multiple_of((me ^ bits) * piece, LANES)
            mixed[:, pl.ds(start, piece)] = rounded(block)
    level = side[:, 0:model_width] + mixed[...]
    resid[...] = level
    scale = lax.rsqrt(jnp.mean(level * level, axis=-1, keepdims=True) + EPS)
    moe_in = (level * scale * side[:, model_width : 2 * model_width]).astype(BF16)
    chips, rows_pad, packed = outgoing.shape
    main = packed - LANES
    tail = moe_in.shape[1] - main
    contract = (((0,), (0,)), ((), ()))

    def gathered(number, values):
        pick = select[:, number * 2 * rows_pad : (number + 1) * 2 * rows_pad].astype(BF16)
        return lax.dot_general(pick, values, contract, preferred_element_type=F32)

    parts = []
    if tail:
        for j in range(main // tail):
            parts.append(gathered(0, moe_in[:, j * tail : (j + 1) * tail]) + gathered(1 + j, moe_in[:, main:]))
    else:
        parts.append(gathered(0, moe_in))
    parts.append(gathered(0, extra))
    low = 0
    for value in parts:
        high = low + value.shape[1]
        for group in range(2):
            body = value[group * rows_pad : (group + 1) * rows_pad].astype(BF16)
            for c in range(chips // 2):
                outgoing[group * (chips // 2) + c, :, low:high] = body
        low = high


def routing_kernel(
    group_width, limit, rows_pad, tails,
    ingate_bias, forget_bias, index, weights, tokens, gain, normalizer, stabilizer,
    select, side, small,
):
    chosen, rows = index.shape
    heads, dim = normalizer.shape[1:]
    width = tokens.shape[1]
    stream = tokens[...].astype(F32)
    scale = lax.rsqrt(jnp.mean(stream * stream, axis=-1, keepdims=True) + EPS)
    side[:, 0:width] = stream
    side[:, width : 2 * width] = jnp.broadcast_to(gain[...], (rows, width))
    low = 2 * width
    for h in range(heads):
        side[:, low : low + dim] = normalizer[:, h, :]
        low += dim
    side[:, low : low + LANES] = jnp.broadcast_to(scale, (rows, LANES))
    small[...] = jnp.zeros_like(small)
    small[0:chosen, 0:rows] = index[...].astype(F32)
    small[64 : 64 + chosen, 0:rows] = weights[...]
    small[32 : 32 + heads, 0:rows] = stabilizer[...]
    for h in range(heads):
        small[40 + h : 41 + h, :] = jnp.full((1, LANES), ingate_bias[h], F32)
        small[48 + h : 49 + h, :] = jnp.full((1, LANES), forget_bias[h], F32)
    flat = small[...].T
    experts = flat[0:rows, :]
    second = (experts[:, 0:1] >= group_width).astype(F32)
    row = lax.broadcasted_iota(jnp.int32, (rows, rows), 0)
    col = lax.broadcasted_iota(jnp.int32, (rows, rows), 1)
    earlier = (col < row).astype(F32)
    before = jnp.dot(earlier, jnp.broadcast_to(second, (rows, LANES)), preferred_element_type=F32)
    place = lax.broadcasted_iota(jnp.int32, (rows, LANES), 0).astype(F32)
    rank = jnp.where(second > 0.5, before, place - before)
    lane = lax.broadcasted_iota(jnp.int32, (rows, LANES), 1).astype(F32)
    base = jnp.where(second > 0.5, float(rows_pad), 0.0)
    chosen_lanes = lane == base + rank
    if tails:
        turn = jnp.zeros_like(rank)
        for q in range(1, limit // tails):
            turn = turn + (rank >= q * tails).astype(F32)
        within = rank - turn * tails
        chosen_lanes = chosen_lanes | (
            lane == (1.0 + within) * (2 * rows_pad) + base + limit + turn
        )
    select[...] = chosen_lanes.astype(F32)
    side[:, low + LANES : low + 2 * LANES] = chosen_lanes.astype(F32)
    side[:, low + 2 * LANES : low + 3 * LANES] = flat[0:rows, :]
    dense = jnp.zeros((rows, LANES), F32)
    for k in range(chosen):
        expert = experts[:, k : k + 1]
        local = jnp.where(expert >= group_width, expert - group_width, expert)
        hit = (lane == local) | (lane == local + group_width)
        dense = dense + jnp.where(hit, flat[0:rows, 64 + k : 65 + k], 0.0)
    high = rounded(dense)
    side[:, low + 3 * LANES : low + 4 * LANES] = jnp.where(lane < group_width, high, dense - high)


def sorted_rows(count, rows_pad, limit, tails, j, back):
    row = lax.broadcasted_iota(jnp.int32, (count, count), 0)
    col = lax.broadcasted_iota(jnp.int32, (count, count), 1)
    spare, real = (row, col) if back else (col, row)
    same = (spare // rows_pad) == (real // rows_pad)
    spare, real = spare % rows_pad, real % rows_pad
    hit = same & (spare >= limit) & (real == (spare - limit) * tails + j) & (real < limit)
    return jnp.where(hit, 1.0, 0.0).astype(BF16)


def expert_kernel(
    group_width, rows_pad, limit, tails, rows_in,
    gate0, up0, down0, gate1, up1, down1, out,
):
    count = rows_in.shape[0]
    main = out.shape[1]
    width = gate0.shape[1]
    tail = width - main
    me = lax.axis_index("ep")
    x = rows_in[:, :main]
    if tail:
        end = None
        for j in range(tails):
            move = sorted_rows(count, rows_pad, limit, tails, j, False)
            term = jnp.dot(move, rows_in[:, j * tail : (j + 1) * tail], preferred_element_type=F32)
            end = term if end is None else end + term
        x = jnp.concatenate((x, end.astype(BF16)), axis=1)
    info = rows_in[:, main:].astype(F32)
    lane = lax.broadcasted_iota(jnp.int32, info.shape, 1)
    inners = []
    weights = []
    for bit, (gate_weight, up_weight) in enumerate(((gate0, up0), (gate1, up1))):
        mine = (me ^ bit) % group_width
        hit = (lane == mine) | (lane == mine + group_width)
        weights.append(jnp.sum(jnp.where(hit, info, 0.0), axis=1, keepdims=True))
        gate = jnp.dot(x, gate_weight[0], preferred_element_type=F32)
        upward = jnp.dot(x, up_weight[0], preferred_element_type=F32)
        inners.append((gate / (1.0 + jnp.exp(-gate)) * upward).astype(BF16))

    def result(low, high):
        total = 0.0
        for inner, down, weight in zip(inners, (down0, down1), weights):
            total = total + weight * jnp.dot(inner, down[0, :, low:high], preferred_element_type=F32)
        return total.astype(BF16)

    if not tail:
        step = 4 * LANES
        for low in range(0, width, step):
            out[:, low : low + step] = result(low, low + step)
        return
    end = result(main, width)
    place = lax.broadcasted_iota(jnp.int32, (count, tail), 0) % rows_pad
    for j in range(tails):
        low, high = j * tail, (j + 1) * tail
        move = sorted_rows(count, rows_pad, limit, tails, j, True)
        moved = jnp.dot(move, end, preferred_element_type=F32)
        body = result(low, high).astype(F32)
        out[:, low:high] = jnp.where(place < limit, body, moved).astype(BF16)


def final_kernel(tails, returned, select, resid_far, out, resid, sem):
    chips, rows_pad, main = returned.shape
    copy = pltpu.make_async_copy(resid_far, resid, sem)
    copy.start()
    tail = out.shape[1] - main
    sums = []
    for group in range(2):
        base = group * (chips // 2)
        total = returned[base].astype(F32)
        for c in range(1, chips // 2):
            total = total + returned[base + c].astype(F32)
        sums.append(total)
    combined = jnp.concatenate(sums, axis=0)
    high = combined.astype(BF16)
    low = (combined - high.astype(F32)).astype(BF16)

    def picked(number, cut):
        pick = select[:, number * 2 * rows_pad : (number + 1) * 2 * rows_pad].astype(BF16)
        return jnp.dot(pick, high[:, cut], preferred_element_type=F32) + jnp.dot(
            pick, low[:, cut], preferred_element_type=F32
        )

    copy.wait()
    out[:, :main] = (resid[:, :main] + picked(0, slice(0, main))).astype(BF16)
    if tail:
        end = resid[:, main:]
        for j in range(tails):
            end = end + picked(1 + j, slice(j * tail, (j + 1) * tail))
        out[:, main:] = end.astype(BF16)


def on_device_fast(
    tokens,
    norm_gain,
    query_weight,
    key_weight,
    value_weight,
    outgate_weight,
    ingate_weight,
    forget_weight,
    ingate_bias,
    forget_bias,
    memory,
    normalizer,
    stabilizer,
    mixer_weight,
    moe_gain,
    expert_gate,
    expert_up,
    expert_down,
    expert_index,
    route_weights,
):
    ep_size = lax.axis_size("ep")
    seq_count, model_width = tokens.shape
    depth, cell_width = query_weight.shape
    stations = ep_size // 4
    chips = ep_size // 2
    z_groups = [[k + 4 * z for z in range(stations)] for k in range(4)]
    chip_groups = [[k + 2 * c for c in range(chips)] for k in range(2)]
    expert_count = ep_size * expert_gate.shape[0]
    group_width = expert_count // 2
    chosen_k = expert_index.shape[1]
    capacity = max(2, ((seq_count + 1) // 2 * chosen_k + group_width - 1) // group_width)
    limit = min(seq_count, capacity * group_width // chosen_k)
    rows = -(-limit // 8) * 8
    spare = rows - limit
    tails = limit // spare if spare and limit % spare == 0 else 0
    if tails and (model_width % (tails + 1) or model_width // (tails + 1) % LANES):
        tails = 0
    if (tails + 1) * 2 * rows > LANES:
        tails = 0
    main = model_width - model_width // (tails + 1) if tails else model_width

    pieces, bits_of = mixer_weight[None], [0]
    batches = []
    bit = 4
    while bit < ep_size:
        moved = swap(pieces, bit)
        moved_bits = [b ^ bit for b in bits_of]
        if 2 * bit < ep_size:
            pieces = stack(pieces, moved)
            bits_of = bits_of + moved_bits
        else:
            batches = [(pieces, bits_of), (moved, moved_bits)]
        bit *= 2

    wide = 4 * cell_width + LANES
    joined, columns = local_call(
        join_kernel,
        [((depth, wide), BF16), ((stations, seq_count, model_width // stations), BF16)],
        scratch=[
            pltpu.VMEM((LANES, depth), F32),
            pltpu.VMEM(tokens.shape, BF16),
            pltpu.VMEM((2, ingate_weight.shape[1], depth), BF16),
            pltpu.SemaphoreType.DMA((7,)),
        ],
        hbm=tuple(range(7)),
        limit=60,
        moved=2 * depth * wide * 2,
    )(tokens, query_weight, key_weight, value_weight, outgate_weight, ingate_weight.T, forget_weight.T)
    joined_y = swap(joined, 2)
    joined_c = swap(joined, 1)
    joined_yc = swap(joined_y, 1)
    columns = lax.all_to_all(columns, "ep", 0, 0, tiled=True, axis_index_groups=z_groups)
    project_options = dict(
        scratch=[pltpu.VMEM((stations * seq_count, 4 * depth), F32)],
        flops=2 * stations * seq_count * 2 * depth * wide,
        moved=2 * depth * wide * 2,
    )
    (near,) = local_call(
        functools.partial(project_kernel, (0, 1)),
        [((stations * seq_count, wide), F32)],
        **project_options,
    )(columns, norm_gain[None], joined, joined_c)
    (partial,) = local_call(
        functools.partial(project_kernel, (2, 3)),
        [((stations, seq_count, wide), BF16)],
        **project_options,
    )(columns, norm_gain[None], joined_y, joined_yc, near)
    received = lax.all_to_all(partial, "ep", 0, 0, tiled=True, axis_index_groups=z_groups)
    for batch, bits in list(batches):
        batches.append((swap(batch, 2), [b ^ 2 for b in bits]))
    for batch, bits in list(batches):
        batches.append((swap(batch, 1), [b ^ 1 for b in bits]))
    blocks = [batch for batch, _ in batches]
    places = tuple(tuple(bits) for _, bits in batches)

    select, side = local_call(
        functools.partial(routing_kernel, group_width, limit, rows, tails),
        [((seq_count, LANES), F32), ((seq_count, 2 * model_width + cell_width + 4 * LANES), F32)],
        scratch=[pltpu.VMEM((LANES, LANES), F32)],
        smem=(0, 1),
    )(
        ingate_bias, forget_bias, expert_index.T, route_weights.T, tokens, moe_gain[None],
        normalizer, stabilizer.T,
    )

    others = []
    for weight in (expert_gate, expert_up, expert_down):
        others.append(swap(weight, 1))

    heads = memory.shape[1]
    new_memory, new_normalizer, new_stabilizer, cell_out = local_call(
        cell_kernel,
        [
            (memory.shape, F32),
            (normalizer.shape, F32),
            (stabilizer.shape, F32),
            ((seq_count, cell_width), BF16),
        ],
        scratch=[
            pltpu.VMEM((heads, LANES, LANES), F32),
            pltpu.VMEM((heads, LANES, LANES), BF16),
            pltpu.VMEM((heads, 64, 2 * LANES), F32),
            pltpu.VMEM((seq_count, cell_width), F32),
            pltpu.VMEM((seq_count, cell_width), F32),
            pltpu.VMEM(memory.shape, F32),
            pltpu.SemaphoreType.DMA((seq_count,)),
        ],
        outs_hbm=(0,),
        flops=4096 * memory.size,
        moved=8 * memory.size,
        limit=16,
    )(received, memory, side)
    resid, outgoing = local_call(
        functools.partial(mix_kernel, places),
        [((seq_count, model_width), F32), ((chips, rows, main + LANES), BF16)],
        scratch=[pltpu.VMEM((seq_count, model_width), F32)],
        flops=4096 * memory.size,
        moved=2 * cell_width * model_width,
        limit=12,
    )(cell_out, side, *blocks)

    direct = lax.all_to_all(
        outgoing, "ep", 0, 0, tiled=True, axis_index_groups=chip_groups
    )
    (summed,) = local_call(
        functools.partial(expert_kernel, group_width, rows, limit, tails),
        [((chips * rows, main), BF16)],
        flops=6 * 2 * chips * rows * model_width * expert_gate.shape[2],
        moved=6 * model_width * expert_gate.shape[2],
        limit=12,
    )(direct.reshape(chips * rows, main + LANES), expert_gate, expert_up, expert_down, *others)
    returned = lax.all_to_all(
        summed.reshape(chips, rows, main), "ep", 0, 0, tiled=True, axis_index_groups=chip_groups
    )
    (layer_out,) = local_call(
        functools.partial(final_kernel, tails),
        [((seq_count, model_width), BF16)],
        scratch=[pltpu.VMEM((seq_count, model_width), F32), pltpu.SemaphoreType.DMA(())],
        anywhere=(2,),
    )(returned, select, resid)
    return (layer_out, new_memory, new_normalizer, new_stabilizer)


def solution(mesh):
    ep_size = mesh.shape["ep"]
    aligned = ep_size % 8 == 0 and ep_size <= 16

    def run(*arrays):
        fits = aligned and arrays[13].shape[1] // ep_size % 128 == 0 and arrays[15].shape[0] == ep_size
        fits = fits and arrays[2].shape[0] // ep_size % 128 == 0 and arrays[10].shape[2] == 128

        def body(*blocks):
            return (on_device_fast if fits else on_device_general)(*blocks)

        step = jax.shard_map(
            body, mesh=mesh, in_specs=ARG_SPECS, out_specs=OUT_SPECS, check_vma=False
        )
        return step(*arrays)

    return run
```

```python
import functools

import jax
import jax.numpy as jnp
from jax import lax
from jax.experimental import pallas as pl
from jax.experimental.pallas import tpu as pltpu
from jax.sharding import PartitionSpec as P


M_HEAD_DIM = 128


EPS = 1e-06


def rms_normed(values, gain):
    scale = lax.rsqrt(jnp.mean(values * values, axis=-1, keepdims=True) + EPS)
    return values * scale * gain


def on_device_general(
    tokens,
    norm_gain,
    query_weight,
    key_weight,
    value_weight,
    outgate_weight,
    ingate_weight,
    forget_weight,
    ingate_bias,
    forget_bias,
    memory,
    normalizer,
    stabilizer,
    mixer_weight,
    moe_gain,
    expert_gate,
    expert_up,
    expert_down,
    expert_index,
    route_weights,
):
    f32 = jnp.float32
    bf16 = jnp.bfloat16
    ep_size = lax.axis_size("ep")
    seq_count = tokens.shape[0]
    model_width = tokens.shape[1]
    cell_width = query_weight.shape[1]
    head_count = ingate_bias.shape[0]
    stream = tokens.astype(f32)
    weight_list = (
        query_weight,
        key_weight,
        value_weight,
        outgate_weight,
        ingate_weight,
        forget_weight,
    )
    normed = rms_normed(stream, norm_gain).astype(bf16)
    normed_cols = lax.all_to_all(normed, "ep", split_axis=1, concat_axis=0, tiled=True)
    joined = jnp.concatenate(weight_list, axis=1)
    projected = lax.psum_scatter(
        jnp.dot(normed_cols, joined, preferred_element_type=f32),
        "ep",
        scatter_dimension=0,
        tiled=True,
    )
    query_sum = projected[:, :cell_width]
    key_sum = projected[:, cell_width : 2 * cell_width]
    value_sum = projected[:, 2 * cell_width : 3 * cell_width]
    outgate_sum = projected[:, 3 * cell_width : 4 * cell_width]
    ingate_sum = projected[:, 4 * cell_width : 4 * cell_width + head_count]
    forget_sum = projected[:, 4 * cell_width + head_count :]
    shape = (seq_count, head_count, M_HEAD_DIM)
    query_heads = query_sum.astype(bf16).astype(f32).reshape(shape)
    key_heads = key_sum.astype(bf16).astype(f32).reshape(shape) * M_HEAD_DIM ** (-0.5)
    value_heads = value_sum.astype(bf16).astype(f32).reshape(shape)
    outgate = outgate_sum.astype(bf16).astype(f32)
    ingate_pre = ingate_sum + ingate_bias
    forget_pre = forget_sum + forget_bias
    log_forget = jax.nn.log_sigmoid(forget_pre)
    new_stabilizer = jnp.maximum(log_forget + stabilizer, ingate_pre)
    keep = jnp.exp(log_forget + stabilizer - new_stabilizer)
    write = jnp.exp(ingate_pre - new_stabilizer)
    new_memory = (
        keep[..., None, None] * memory
        + write[..., None, None] * key_heads[..., :, None] * value_heads[..., None, :]
    )
    new_normalizer = keep[..., None] * normalizer + write[..., None] * key_heads
    numer = jnp.einsum("thd,thde->the", query_heads, new_memory, precision=lax.Precision.HIGHEST)
    denom = jnp.sum(query_heads * new_normalizer, axis=-1)
    hidden = numer / jnp.maximum(jnp.abs(denom), 1.0)[..., None]
    cell_out = (hidden.reshape(seq_count, cell_width) * jax.nn.sigmoid(outgate)).astype(bf16)
    mixed_cols = jnp.dot(
        lax.all_gather(cell_out, "ep", axis=0, tiled=True), mixer_weight, preferred_element_type=f32
    ).astype(bf16)
    mixed = lax.all_to_all(mixed_cols, "ep", split_axis=0, concat_axis=1, tiled=True)
    resid = stream + mixed.astype(f32)
    moe_in = rms_normed(resid, moe_gain).astype(bf16)
    local_experts = expert_gate.shape[0]
    expert_count = local_experts * ep_size
    chosen_k = expert_index.shape[1]
    group_width = expert_count // 2
    capacity = max(2, ((seq_count + 1) // 2 * chosen_k + group_width - 1) // group_width)
    routes = expert_index.reshape(-1)
    matches = (routes[:, None] == jnp.arange(expert_count, dtype=jnp.int32)[None, :]).astype(
        jnp.int32
    )
    slots = jnp.sum((jnp.cumsum(matches, axis=0) - 1) * matches, axis=1)
    target = routes * capacity + slots
    placing = (
        jnp.arange(expert_count * capacity, dtype=jnp.int32)[:, None] == target[None, :]
    ).astype(bf16)
    route_rows = jnp.repeat(moe_in, chosen_k, axis=0)
    outgoing = jnp.dot(placing, route_rows, preferred_element_type=f32).astype(bf16)
    outgoing = outgoing.reshape(expert_count, capacity, model_width)
    received = lax.all_to_all(outgoing, "ep", split_axis=0, concat_axis=0, tiled=True)
    count = received.shape[1]
    grouped = received.reshape(ep_size, local_experts, count, model_width)
    gate = jnp.einsum("sxcd,xdf->sxcf", grouped, expert_gate, preferred_element_type=f32)
    upward = jnp.einsum("sxcd,xdf->sxcf", grouped, expert_up, preferred_element_type=f32)
    inner = (jax.nn.silu(gate) * upward).astype(bf16)
    result = jnp.einsum("sxcf,xfd->sxcd", inner, expert_down, preferred_element_type=f32).astype(
        bf16
    )
    result = result.reshape(ep_size * local_experts, count, model_width)
    returned = lax.all_to_all(result, "ep", split_axis=0, concat_axis=0, tiled=True)
    flat_back = returned.reshape(expert_count * capacity, model_width)
    picked = jnp.dot(placing.T, flat_back, preferred_element_type=f32)
    weighted = picked * route_weights.reshape(-1)[:, None]
    combined = jnp.sum(weighted.reshape(seq_count, chosen_k, model_width), axis=1)
    layer_out = (resid + combined).astype(bf16)
    return (layer_out, new_memory, new_normalizer, new_stabilizer)


ARG_SPECS = (
    P(("grp", "ep"), None),
    P(),
    P("ep", None),
    P("ep", None),
    P("ep", None),
    P("ep", None),
    P("ep", None),
    P("ep", None),
    P(),
    P(),
    P(("grp", "ep"), None, None, None),
    P(("grp", "ep"), None, None),
    P(("grp", "ep"), None),
    P(None, "ep"),
    P(),
    P("ep", None, None),
    P("ep", None, None),
    P("ep", None, None),
    P(("grp", "ep"), None),
    P(("grp", "ep"), None),
)
OUT_SPECS = (
    P(("grp", "ep"), None),
    P(("grp", "ep"), None, None, None),
    P(("grp", "ep"), None, None),
    P(("grp", "ep"), None),
)


def swap(value, bit):
    size = lax.axis_size("ep")
    return lax.ppermute(value, "ep", [(i, i ^ bit) for i in range(size)])


F32 = jnp.float32
BF16 = jnp.bfloat16
LANES = 128


def local_call(kernel, outs, scratch=(), flops=1, moved=1, smem=(), hbm=(), anywhere=(), outs_hbm=(), limit=8):
    def call(*args):
        def space(i):
            if i in smem:
                return pltpu.SMEM
            if i in hbm:
                return pltpu.HBM
            return pl.ANY if i in anywhere else pltpu.VMEM

        specs = [pl.BlockSpec(memory_space=space(i)) for i in range(len(args))]
        return pl.pallas_call(
            kernel,
            out_shape=[jax.ShapeDtypeStruct(*o) for o in outs],
            in_specs=specs,
            out_specs=[
                pl.BlockSpec(memory_space=pltpu.HBM if i in outs_hbm else pltpu.VMEM)
                for i in range(len(outs))
            ],
            scratch_shapes=list(scratch),
            compiler_params=pltpu.CompilerParams(vmem_limit_bytes=int(limit * 2**20)),
            cost_estimate=pl.CostEstimate(
                flops=flops, bytes_accessed=moved, transcendentals=0
            ),
        )(*args)

    return call


def stack_kernel(first, second, out, sems):
    count = first.shape[0]
    copies = [
        pltpu.make_async_copy(first, out.at[:count], sems.at[0]),
        pltpu.make_async_copy(second, out.at[count:], sems.at[1]),
    ]
    for copy in copies:
        copy.start()
    for copy in copies:
        copy.wait()


def stack(first, second):
    shape = (first.shape[0] + second.shape[0],) + first.shape[1:]
    return local_call(
        stack_kernel,
        [(shape, first.dtype)],
        scratch=[pltpu.SemaphoreType.DMA((2,))],
        anywhere=(0, 1),
        limit=60,
        moved=2 * first.size * 4,
    )(first, second)[0]


def join_kernel(
    tokens, query, key, value, outgate, ingate, forget, joined, columns, turned, held, narrow, sems
):
    width = query.shape[1]
    heads = ingate.shape[0]
    copies = [
        pltpu.make_async_copy(ingate, narrow.at[0], sems.at[0]),
        pltpu.make_async_copy(forget, narrow.at[1], sems.at[1]),
        pltpu.make_async_copy(tokens, held, sems.at[2]),
    ]
    for i, ref in enumerate((query, key, value, outgate)):
        copies.append(
            pltpu.make_async_copy(ref, joined.at[:, i * width : (i + 1) * width], sems.at[3 + i])
        )
    for copy in copies:
        copy.start()
    turned[...] = jnp.zeros_like(turned)
    for copy in copies[:3]:
        copy.wait()
    turned[:heads] = narrow[0].astype(F32)
    turned[heads : 2 * heads] = narrow[1].astype(F32)
    joined[:, 4 * width :] = turned[...].T.astype(BF16)
    part = columns.shape[2]
    for z in range(columns.shape[0]):
        columns[z] = held[:, z * part : (z + 1) * part]
    for copy in copies[3:]:
        copy.wait()


def project_kernel(bits_of, columns, gain, first, second, *refs):
    stations, rows, part = columns.shape
    full = rows - 4
    depth = first.shape[0]
    width = first.shape[1]
    before, out, scaled, ends = refs if len(refs) == 4 else (None,) + refs
    me = lax.axis_index("ep")
    station, place = me // 4, me % 4
    gain_here = gain[:, pl.ds(pl.multiple_of(station * part, LANES), part)]
    for z in range(stations):
        x = columns[z].astype(F32) * gain_here
        scaled[z * full : (z + 1) * full, :] = x[:full]
        low = stations * full + z * 8
        scaled[low : low + 4, :] = x[full:]
        scaled[low + 4 : low + 8, :] = x[full:]
    parts = []
    for bits in bits_of:
        start = pl.multiple_of((place ^ bits) * depth, LANES)
        parts.append(scaled[:, pl.ds(start, depth)].astype(BF16))
    step = 4 * LANES
    for low in range(0, width, step):
        high = min(low + step, width)
        term = jnp.dot(parts[0], first[:, low:high], preferred_element_type=F32)
        term = term + jnp.dot(parts[1], second[:, low:high], preferred_element_type=F32)
        if before is None:
            out[:, low:high] = term
            continue
        term = term + before[:, low:high]
        for z in range(stations):
            for f in range(full // 8):
                start = z * full + f * 8
                out[z, :, f * width + low : f * width + high] = term[start : start + 8].astype(BF16)
        ends[:, low:high] = term[stations * full :]
    if before is None:
        return
    split = left_width(width)
    base = full // 8 * width
    upper = lax.broadcasted_iota(jnp.int32, (8, width - split), 0) < 4
    for z in range(stations):
        end = ends[z * 8 : (z + 1) * 8, :]
        paired = jnp.where(upper, end[:, : width - split], end[:, split:])
        out[z, :, base : base + width - split] = paired.astype(BF16)
        out[z, :, base + width - split :] = end[:, width - split : split].astype(BF16)


def left_width(width):
    return -(-width // (2 * LANES)) * LANES


def unpacked(total, rows, width):
    full = rows - 4
    split = left_width(width)
    tiles = [total[:, f * width : (f + 1) * width] for f in range(full // 8)]
    base = full // 8 * width
    left = total[0:4, base : base + split]
    right = total[4:8, base : base + width - split]
    return jnp.concatenate(tiles + [jnp.concatenate((left, right), axis=1)], axis=0)


def rounded(value):
    return value.astype(BF16).astype(F32)


def gate_kernel(
    rows, heads, received, side, new_normalizer, new_stabilizer,
    flipped, spread, keeps, factor, turned, values,
):
    stations = received.shape[0]
    width = keeps.shape[1]
    dim = width // heads
    scale = side[:, width : width + 1]
    known = side[:, width + LANES : width + 2 * LANES]
    total = received[0].astype(F32)
    for z in range(1, stations):
        total = total + received[z].astype(F32)
    total = unpacked(total, rows, 4 * width + LANES) * scale
    gates = total[:, 4 * width :]
    turned[...] = jnp.zeros_like(turned)
    values[...] = jnp.zeros_like(values)
    lane = lax.broadcasted_iota(jnp.int32, (rows, heads), 1)
    states = jnp.zeros((rows, heads), F32)
    for h in range(heads):
        cut = slice(h * dim, (h + 1) * dim)
        query = rounded(total[:, h * dim : (h + 1) * dim])
        key = rounded(total[:, width + h * dim : width + (h + 1) * dim]) * dim ** (-0.5)
        ingate_pre = gates[:, h : h + 1] + known[:, 40 + h : 41 + h]
        forget_pre = gates[:, heads + h : heads + h + 1] + known[:, 48 + h : 49 + h]
        log_forget = jnp.minimum(forget_pre, 0.0) - jnp.log1p(jnp.exp(-jnp.abs(forget_pre)))
        carried = log_forget + known[:, 32 + h : 33 + h]
        state = jnp.maximum(carried, ingate_pre)
        states = jnp.where(lane == h, state, states)
        keep = jnp.broadcast_to(jnp.exp(carried - state), (rows, dim))
        keeps[:, cut] = keep
        write_key = jnp.exp(ingate_pre - state) * key
        normal = keep * side[:, cut] + write_key
        new_normalizer[:, h, :] = normal
        denom = jnp.sum(query * normal, axis=-1, keepdims=True)
        outgate = rounded(total[:, 3 * width + h * dim : 3 * width + (h + 1) * dim])
        factor[:, cut] = 1.0 / (jnp.maximum(jnp.abs(denom), 1.0) * (1.0 + jnp.exp(-outgate)))
        high = rounded(write_key)
        middle = rounded(write_key - high)
        turned[h, 0:rows, :] = query
        turned[h, 16 : 16 + rows, :] = high
        turned[h, 32 : 32 + rows, :] = middle
        turned[h, 48 : 48 + rows, :] = rounded(write_key - high - middle)
        flipped[h] = turned[h].T.astype(BF16)
        value = total[:, 2 * width + h * dim : 2 * width + (h + 1) * dim]
        for i in range(1, 4):
            values[16 * i : 16 * i + rows, :] = value
        spread[h, :, dim:] = values[...].astype(BF16)
        which = lax.broadcasted_iota(jnp.int32, (64, dim), 0)
        spread[h, :, :dim] = jnp.where(which < 16, 1.0, 0.0).astype(BF16)
    new_stabilizer[...] = states


def cell_kernel(
    flipped, spread, keeps, factor, memory, new_memory, cell_out, numer, fresh, sems
):
    rows, heads, dim = memory.shape[:3]
    copies = []
    which = lax.broadcasted_iota(jnp.int32, (64, 2 * dim), 0) % 16
    spreads = [spread[h] for h in range(heads)]
    for t in range(rows):
        for h in range(heads):
            cut = slice(h * dim, (h + 1) * dim)
            row_only = jnp.where(which == t, spreads[h], jnp.zeros_like(spreads[h]))
            both = jnp.dot(flipped[h][:, :64], row_only, preferred_element_type=F32)
            block = keeps[t : t + 1, cut] * memory[t, h] + both[:, dim:]
            fresh[t, h] = block
            numer[t : t + 1, cut] = jnp.sum(both[:, :dim] * block, axis=0, keepdims=True)
        copies.append(pltpu.make_async_copy(fresh.at[t], new_memory.at[t], sems.at[t]))
        copies[-1].start()
    cell_out[...] = (numer[...] * factor[...]).astype(BF16)
    for copy in copies:
        copy.wait()


def mix_kernel(places, cell_out, side, select, tokens, gain, *refs):
    blocks, (resid, outgoing, mixed) = refs[: len(places)], refs[len(places) :]
    cell = cell_out[...]
    extra = side[:, side.shape[1] - LANES :].astype(BF16)
    me = lax.axis_index("ep")
    piece = blocks[0].shape[2]
    for i, bits_of in enumerate(places):
        for number, bits in enumerate(bits_of):
            block = jnp.dot(cell, blocks[i][number], preferred_element_type=F32)
            start = pl.multiple_of((me ^ bits) * piece, LANES)
            mixed[:, pl.ds(start, piece)] = rounded(block)
    level = tokens[...].astype(F32) + mixed[...]
    resid[...] = level
    scale = lax.rsqrt(jnp.mean(level * level, axis=-1, keepdims=True) + EPS)
    moe_in = (level * scale * gain[...]).astype(BF16)
    chips, rows_pad, packed = outgoing.shape
    main = packed - LANES
    tail = moe_in.shape[1] - main
    contract = (((0,), (0,)), ((), ()))

    def gathered(number, values):
        pick = select[:, number * 2 * rows_pad : (number + 1) * 2 * rows_pad].astype(BF16)
        return lax.dot_general(pick, values, contract, preferred_element_type=F32)

    parts = []
    if tail:
        for j in range(main // tail):
            parts.append(gathered(0, moe_in[:, j * tail : (j + 1) * tail]) + gathered(1 + j, moe_in[:, main:]))
    else:
        parts.append(gathered(0, moe_in))
    parts.append(gathered(0, extra))
    low = 0
    for value in parts:
        high = low + value.shape[1]
        for group in range(2):
            body = value[group * rows_pad : (group + 1) * rows_pad].astype(BF16)
            for c in range(chips // 2):
                outgoing[group * (chips // 2) + c, :, low:high] = body
        low = high


def routing_kernel(
    group_width, limit, rows_pad, tails,
    ingate_bias, forget_bias, index, weights, tokens, normalizer, stabilizer,
    select, side, small,
):
    chosen, rows = index.shape
    heads, dim = normalizer.shape[1:]
    stream = tokens[...].astype(F32)
    scale = lax.rsqrt(jnp.mean(stream * stream, axis=-1, keepdims=True) + EPS)
    low = 0
    for h in range(heads):
        side[:, low : low + dim] = normalizer[:, h, :]
        low += dim
    side[:, low : low + LANES] = jnp.broadcast_to(scale, (rows, LANES))
    small[...] = jnp.zeros_like(small)
    small[0:chosen, 0:rows] = index[...].astype(F32)
    small[64 : 64 + chosen, 0:rows] = weights[...]
    small[32 : 32 + heads, 0:rows] = stabilizer[...]
    for h in range(heads):
        small[40 + h : 41 + h, :] = jnp.full((1, LANES), ingate_bias[h], F32)
        small[48 + h : 49 + h, :] = jnp.full((1, LANES), forget_bias[h], F32)
    flat = small[...].T
    experts = flat[0:rows, :]
    second = (experts[:, 0:1] >= group_width).astype(F32)
    row = lax.broadcasted_iota(jnp.int32, (rows, rows), 0)
    col = lax.broadcasted_iota(jnp.int32, (rows, rows), 1)
    earlier = (col < row).astype(F32)
    before = jnp.dot(earlier, jnp.broadcast_to(second, (rows, LANES)), preferred_element_type=F32)
    place = lax.broadcasted_iota(jnp.int32, (rows, LANES), 0).astype(F32)
    rank = jnp.where(second > 0.5, before, place - before)
    lane = lax.broadcasted_iota(jnp.int32, (rows, LANES), 1).astype(F32)
    base = jnp.where(second > 0.5, float(rows_pad), 0.0)
    chosen_lanes = lane == base + rank
    if tails:
        turn = jnp.zeros_like(rank)
        for q in range(1, limit // tails):
            turn = turn + (rank >= q * tails).astype(F32)
        within = rank - turn * tails
        chosen_lanes = chosen_lanes | (
            lane == (1.0 + within) * (2 * rows_pad) + base + limit + turn
        )
    select[...] = chosen_lanes.astype(F32)
    side[:, low + LANES : low + 2 * LANES] = flat[0:rows, :]
    dense = jnp.zeros((rows, LANES), F32)
    for k in range(chosen):
        expert = experts[:, k : k + 1]
        local = jnp.where(expert >= group_width, expert - group_width, expert)
        hit = (lane == local) | (lane == local + group_width)
        dense = dense + jnp.where(hit, flat[0:rows, 64 + k : 65 + k], 0.0)
    high = rounded(dense)
    side[:, low + 2 * LANES : low + 3 * LANES] = jnp.where(lane < group_width, high, dense - high)


def sorted_rows(count, rows_pad, limit, tails, j, back):
    row = lax.broadcasted_iota(jnp.int32, (count, count), 0)
    col = lax.broadcasted_iota(jnp.int32, (count, count), 1)
    spare, real = (row, col) if back else (col, row)
    same = (spare // rows_pad) == (real // rows_pad)
    spare, real = spare % rows_pad, real % rows_pad
    hit = same & (spare >= limit) & (real == (spare - limit) * tails + j) & (real < limit)
    return jnp.where(hit, 1.0, 0.0).astype(BF16)


def expert_kernel(
    group_width, rows_pad, limit, tails, rows_in,
    gate0, up0, down0, gate1, up1, down1, out,
):
    count = rows_in.shape[0]
    main = out.shape[1]
    width = gate0.shape[1]
    tail = width - main
    me = lax.axis_index("ep")
    x = rows_in[:, :main]
    if tail:
        end = None
        for j in range(tails):
            move = sorted_rows(count, rows_pad, limit, tails, j, False)
            term = jnp.dot(move, rows_in[:, j * tail : (j + 1) * tail], preferred_element_type=F32)
            end = term if end is None else end + term
        x = jnp.concatenate((x, end.astype(BF16)), axis=1)
    info = rows_in[:, main:].astype(F32)
    lane = lax.broadcasted_iota(jnp.int32, info.shape, 1)
    inners = []
    weights = []
    for bit, (gate_weight, up_weight) in enumerate(((gate0, up0), (gate1, up1))):
        mine = (me ^ bit) % group_width
        hit = (lane == mine) | (lane == mine + group_width)
        weights.append(jnp.sum(jnp.where(hit, info, 0.0), axis=1, keepdims=True))
        gate = jnp.dot(x, gate_weight[0], preferred_element_type=F32)
        upward = jnp.dot(x, up_weight[0], preferred_element_type=F32)
        inners.append((gate / (1.0 + jnp.exp(-gate)) * upward).astype(BF16))

    def result(low, high):
        total = 0.0
        for inner, down, weight in zip(inners, (down0, down1), weights):
            total = total + weight * jnp.dot(inner, down[0, :, low:high], preferred_element_type=F32)
        return total.astype(BF16)

    if not tail:
        step = 4 * LANES
        for low in range(0, width, step):
            out[:, low : low + step] = result(low, low + step)
        return
    end = result(main, width)
    place = lax.broadcasted_iota(jnp.int32, (count, tail), 0) % rows_pad
    for j in range(tails):
        low, high = j * tail, (j + 1) * tail
        move = sorted_rows(count, rows_pad, limit, tails, j, True)
        moved = jnp.dot(move, end, preferred_element_type=F32)
        body = result(low, high).astype(F32)
        out[:, low:high] = jnp.where(place < limit, body, moved).astype(BF16)


def final_kernel(tails, returned, select, resid_far, out, resid, sem):
    chips, rows_pad, main = returned.shape
    copy = pltpu.make_async_copy(resid_far, resid, sem)
    copy.start()
    tail = out.shape[1] - main
    sums = []
    for group in range(2):
        base = group * (chips // 2)
        total = returned[base].astype(F32)
        for c in range(1, chips // 2):
            total = total + returned[base + c].astype(F32)
        sums.append(total)
    combined = jnp.concatenate(sums, axis=0)
    high = combined.astype(BF16)
    low = (combined - high.astype(F32)).astype(BF16)

    def picked(number, cut):
        pick = select[:, number * 2 * rows_pad : (number + 1) * 2 * rows_pad].astype(BF16)
        return jnp.dot(pick, high[:, cut], preferred_element_type=F32) + jnp.dot(
            pick, low[:, cut], preferred_element_type=F32
        )

    copy.wait()
    out[:, :main] = (resid[:, :main] + picked(0, slice(0, main))).astype(BF16)
    if tail:
        end = resid[:, main:]
        for j in range(tails):
            end = end + picked(1 + j, slice(j * tail, (j + 1) * tail))
        out[:, main:] = end.astype(BF16)


def on_device_fast(
    tokens,
    norm_gain,
    query_weight,
    key_weight,
    value_weight,
    outgate_weight,
    ingate_weight,
    forget_weight,
    ingate_bias,
    forget_bias,
    memory,
    normalizer,
    stabilizer,
    mixer_weight,
    moe_gain,
    expert_gate,
    expert_up,
    expert_down,
    expert_index,
    route_weights,
):
    ep_size = lax.axis_size("ep")
    seq_count, model_width = tokens.shape
    depth, cell_width = query_weight.shape
    stations = ep_size // 4
    chips = ep_size // 2
    z_groups = [[k + 4 * z for z in range(stations)] for k in range(4)]
    chip_groups = [[k + 2 * c for c in range(chips)] for k in range(2)]
    expert_count = ep_size * expert_gate.shape[0]
    group_width = expert_count // 2
    chosen_k = expert_index.shape[1]
    capacity = max(2, ((seq_count + 1) // 2 * chosen_k + group_width - 1) // group_width)
    limit = min(seq_count, capacity * group_width // chosen_k)
    rows = -(-limit // 8) * 8
    spare = rows - limit
    tails = limit // spare if spare and limit % spare == 0 else 0
    if tails and (model_width % (tails + 1) or model_width // (tails + 1) % LANES):
        tails = 0
    if (tails + 1) * 2 * rows > LANES:
        tails = 0
    main = model_width - model_width // (tails + 1) if tails else model_width

    pieces, bits_of = mixer_weight[None], [0]
    batches = []
    bit = 4
    while bit < ep_size:
        moved = swap(pieces, bit)
        moved_bits = [b ^ bit for b in bits_of]
        if 2 * bit < ep_size:
            pieces = stack(pieces, moved)
            bits_of = bits_of + moved_bits
        else:
            batches = [(pieces, bits_of), (moved, moved_bits)]
        bit *= 2

    wide = 4 * cell_width + LANES
    joined, columns = local_call(
        join_kernel,
        [((depth, wide), BF16), ((stations, seq_count, model_width // stations), BF16)],
        scratch=[
            pltpu.VMEM((LANES, depth), F32),
            pltpu.VMEM(tokens.shape, BF16),
            pltpu.VMEM((2, ingate_weight.shape[1], depth), BF16),
            pltpu.SemaphoreType.DMA((7,)),
        ],
        hbm=tuple(range(7)),
        limit=60,
        moved=2 * depth * wide * 2,
    )(tokens, query_weight, key_weight, value_weight, outgate_weight, ingate_weight.T, forget_weight.T)
    joined_y = swap(joined, 2)
    joined_c = swap(joined, 1)
    joined_yc = swap(joined_y, 1)
    columns = lax.all_to_all(columns, "ep", 0, 0, tiled=True, axis_index_groups=z_groups)
    message = (seq_count - 4) // 8 * wide + left_width(wide)
    project_rows = stations * (seq_count + 4)
    project_options = dict(
        scratch=[
            pltpu.VMEM((project_rows, 4 * depth), F32),
            pltpu.VMEM((stations * 8, wide), F32),
        ],
        flops=2 * stations * seq_count * 2 * depth * wide,
        moved=2 * depth * wide * 2,
    )
    (near,) = local_call(
        functools.partial(project_kernel, (0, 1)),
        [((project_rows, wide), F32)],
        **project_options,
    )(columns, norm_gain[None], joined, joined_c)
    (partial,) = local_call(
        functools.partial(project_kernel, (2, 3)),
        [((stations, 8, message), BF16)],
        **project_options,
    )(columns, norm_gain[None], joined_y, joined_yc, near)
    received = lax.all_to_all(partial, "ep", 0, 0, tiled=True, axis_index_groups=z_groups)
    for batch, bits in list(batches):
        batches.append((swap(batch, 2), [b ^ 2 for b in bits]))
    for batch, bits in list(batches):
        batches.append((swap(batch, 1), [b ^ 1 for b in bits]))
    blocks = [batch for batch, _ in batches]
    places = tuple(tuple(bits) for _, bits in batches)

    select, side = local_call(
        functools.partial(routing_kernel, group_width, limit, rows, tails),
        [
            ((seq_count, LANES), F32),
            ((seq_count, cell_width + 3 * LANES), F32),
        ],
        scratch=[pltpu.VMEM((LANES, LANES), F32)],
        smem=(0, 1),
    )(
        ingate_bias, forget_bias, expert_index.T, route_weights.T, tokens,
        normalizer, stabilizer.T,
    )

    others = []
    for weight in (expert_gate, expert_up, expert_down):
        others.append(swap(weight, 1))

    heads = memory.shape[1]
    new_normalizer, new_stabilizer, *turned = local_call(
        functools.partial(gate_kernel, seq_count, heads),
        [
            (normalizer.shape, F32),
            (stabilizer.shape, F32),
            ((heads, LANES, LANES), BF16),
            ((heads, 64, 2 * LANES), BF16),
            ((seq_count, cell_width), F32),
            ((seq_count, cell_width), F32),
        ],
        scratch=[
            pltpu.VMEM((heads, LANES, LANES), F32),
            pltpu.VMEM((64, LANES), F32),
        ],
        flops=4096 * memory.size,
    )(received, side)
    new_memory, cell_out = local_call(
        cell_kernel,
        [(memory.shape, F32), ((seq_count, cell_width), BF16)],
        scratch=[
            pltpu.VMEM((seq_count, cell_width), F32),
            pltpu.VMEM(memory.shape, F32),
            pltpu.SemaphoreType.DMA((seq_count,)),
        ],
        outs_hbm=(0,),
        flops=4096 * memory.size,
        moved=8 * memory.size,
        limit=12,
    )(*turned, memory)
    resid, outgoing = local_call(
        functools.partial(mix_kernel, places),
        [((seq_count, model_width), F32), ((chips, rows, main + LANES), BF16)],
        scratch=[pltpu.VMEM((seq_count, model_width), F32)],
        flops=4096 * memory.size,
        moved=2 * cell_width * model_width,
        limit=12,
    )(cell_out, side, select, tokens, moe_gain[None], *blocks)

    direct = lax.all_to_all(
        outgoing, "ep", 0, 0, tiled=True, axis_index_groups=chip_groups
    )
    (summed,) = local_call(
        functools.partial(expert_kernel, group_width, rows, limit, tails),
        [((chips * rows, main), BF16)],
        flops=6 * 2 * chips * rows * model_width * expert_gate.shape[2],
        moved=6 * model_width * expert_gate.shape[2],
        limit=12,
    )(direct.reshape(chips * rows, main + LANES), expert_gate, expert_up, expert_down, *others)
    returned = lax.all_to_all(
        summed.reshape(chips, rows, main), "ep", 0, 0, tiled=True, axis_index_groups=chip_groups
    )
    (layer_out,) = local_call(
        functools.partial(final_kernel, tails),
        [((seq_count, model_width), BF16)],
        scratch=[pltpu.VMEM((seq_count, model_width), F32), pltpu.SemaphoreType.DMA(())],
        anywhere=(2,),
    )(returned, select, resid)
    return (layer_out, new_memory, new_normalizer, new_stabilizer)


def solution(mesh):
    ep_size = mesh.shape["ep"]
    aligned = ep_size % 8 == 0 and ep_size <= 16

    def run(*arrays):
        fits = aligned and arrays[0].shape[0] // mesh.size % 8 == 4
        fits = fits and arrays[13].shape[1] // ep_size % 128 == 0 and arrays[15].shape[0] == ep_size
        fits = fits and arrays[2].shape[0] // ep_size % 128 == 0 and arrays[10].shape[2] == 128

        def body(*blocks):
            return (on_device_fast if fits else on_device_general)(*blocks)

        step = jax.shard_map(
            body, mesh=mesh, in_specs=ARG_SPECS, out_specs=OUT_SPECS, check_vma=False
        )
        return step(*arrays)

    return run
```
